128 devices in a mesh: sp: 16 (over z, x), dp: 8 (over y, core).
Axes of the slice: x: 4, y: 4, z: 4, core: 2. Of those that a mesh axis runs over, the one named last changes fastest.
Arguments:
- residual_in: bfloat16 [8, 2048, 2048], P('dp', 'sp'), may hold values from -6 to 6
- query_proj: bfloat16 [8, 2048, 2048], P('dp', 'sp'), may hold values from -8 to 8
- key_proj: bfloat16 [8, 2048, 512], P('dp', 'sp'), may hold values from -8 to 8
- value_proj: bfloat16 [8, 2048, 512], P('dp', 'sp'), may hold values from -6 to 6
- query_gain: float32 [128], replicated, may hold values from 0.1 to 7
- key_gain: float32 [128], replicated, may hold values from 0.1 to 7
- out_weight: bfloat16 [2048, 2048], replicated, may hold values from -0.125 to 0.125
- post_gain: float32 [2048], replicated, may hold values from 0.1 to 1.9
- pre_gain: float32 [2048], replicated, may hold values from 0.1 to 1.9
- route_ids: int32 [8, 2048, 2], P('dp', 'sp'), may hold values from 0 to 127, as said below
- group_weight: float32 [8, 2048], P('dp', 'sp'), may hold values from 0.25 to 1
- first_share: float32 [8, 2048], P('dp', 'sp'), may hold values from 0.5 to 1
- gate_weight: bfloat16 [128, 2048, 512], P(('sp', 'dp')), may hold values from -0.125 to 0.125
- up_weight: bfloat16 [128, 2048, 512], P(('sp', 'dp')), may hold values from -0.125 to 0.125
- down_weight: bfloat16 [128, 512, 2048], P(('sp', 'dp')), may hold values from -0.25 to 0.25
Outputs:
- layer_out: bfloat16 [8, 2048, 2048], P('dp', 'sp')
The draws below stay inside these ranges and needn't reach their ends.
Inputs may be any that keep to these rules, and one draw needn't show every extreme that they name: `route_ids`: each token names two different experts of one group of 32 consecutive experts. Among the 128 tokens of one device each group is chosen by exactly 32 tokens, no expert is named by more than 4 of them, and in every draw one expert of each group is named by exactly 4 tokens of every device.
All inputs are finite; a program needn't handle non-finite values.
Results may differ from the reference program's by a relative error of at most 0.009.
The reference program's roundings to bfloat16 on the way count: a program that leaves them out, or rounds other values in their place, can miss the bound.
Values may be sent and summed in bfloat16 or wider, within the bound.
No kernel may reach another device: no remote copies, remote signals or barrier semaphores. Data moves between devices by JAX's collectives and lax.ppermute only.
A program may use at most 128 MiB of HBM per device.

```python
import jax
import jax.numpy as jnp
from jax import lax

D = 2048
HEADS = 16
KV_HEADS = 4
HEAD_DIM = 128
FF = 512
GROUPS = 4
GRID_W = 64
TOK_DEV = 128
SEQS = 8
SEQ = 2048
EXPERTS = 128
CAP = 4
N_SP = 16
N_DP = 8


def draw_query_proj(key, part):
    own = jax.random.fold_in(key, 11)
    base = jax.random.truncated_normal(own, -6.0, 6.0, (SEQS, SEQ, HEADS * HEAD_DIM), jnp.float32)
    return base.astype(jnp.bfloat16)


def draw_key_proj(key, part):
    own = jax.random.fold_in(key, 12)
    base = jax.random.truncated_normal(own, -6.0, 6.0, (SEQS, SEQ, KV_HEADS * HEAD_DIM), jnp.float32)
    return base.astype(jnp.bfloat16)


def gain_table(own):
    return 1.0 + 0.18 * jax.random.truncated_normal(own, -5.0, 5.0, (HEAD_DIM,), jnp.float32)


def draw_query_gain(key, part):
    return gain_table(jax.random.fold_in(key, 21))


def draw_key_gain(key, part):
    return gain_table(jax.random.fold_in(key, 22))


def draw_route_ids(key, part):
    per_group = TOK_DEV // GROUPS
    group_width = EXPERTS // GROUPS
    middle = CAP // 2
    hot = jax.random.randint(jax.random.fold_in(key, 31), (GROUPS,), 0, group_width)
    block_count = SEQS * (SEQ // TOK_DEV)

    def one_block(block_key):
        key_tok, key_rest = jax.random.split(block_key)
        order = jax.random.permutation(key_tok, TOK_DEV)
        firsts = []
        seconds = []
        for group_id in range(GROUPS):
            group_key = jax.random.fold_in(key_rest, group_id)
            key_perm, key_shift, key_swap = jax.random.split(group_key, 3)
            shuffled = jax.random.permutation(key_perm, group_width).astype(jnp.int32)
            shifts = jax.random.randint(key_shift, (group_width // 2,), -middle, middle + 1)
            hot_place = jnp.sum(jnp.where(shuffled == hot[group_id], jnp.arange(group_width, dtype=jnp.int32), 0))
            sign_value = 1 - 2 * (hot_place % 2)
            shifts = shifts.at[hot_place // 2].set(middle * sign_value)
            counts = jnp.zeros((group_width,), jnp.int32).at[shuffled[0::2]].set(middle + shifts).at[shuffled[1::2]].set(middle - shifts)
            listed = jnp.repeat(jnp.arange(group_width, dtype=jnp.int32), counts, total_repeat_length=2 * per_group)
            first_pick = listed[:per_group]
            second_pick = listed[per_group:]
            swap_bits = jax.random.randint(key_swap, (per_group,), 0, 2)
            leading = jnp.where(swap_bits == 1, second_pick, first_pick)
            trailing = jnp.where(swap_bits == 1, first_pick, second_pick)
            firsts.append(leading + group_id * group_width)
            seconds.append(trailing + group_id * group_width)
        pairs = jnp.stack([jnp.concatenate(firsts), jnp.concatenate(seconds)], axis=1).astype(jnp.int32)
        return jnp.zeros((TOK_DEV, 2), jnp.int32).at[order].set(pairs)
    blocks_all = jax.vmap(one_block)(jax.random.split(jax.random.fold_in(key, 32), block_count))
    return blocks_all.reshape(SEQS, SEQ, 2)


def level_of(rng, shape, cuts, least, top_value):
    level, own = 1.0, jax.random.fold_in(rng, 6)
    for axis_at, shards_of in cuts:
        steps = jnp.exp(jax.random.uniform(jax.random.fold_in(own, axis_at), (shards_of,), jnp.float32, least / len(cuts), top_value / len(cuts)))
        level = level * jnp.repeat(steps, shape[axis_at] // shards_of).reshape([-1 if axis == axis_at else 1 for axis in range(len(shape))])
    return level


def bell_draw(key, shape, deviation, bound, cuts=(), kind=jnp.bfloat16):
    entries = jax.random.normal(key, shape, jnp.float32) * deviation
    if len(cuts) > 0:
        entries = level_of(key, shape, cuts, -0.22, 0.18) * entries
    return jnp.clip(entries, min=-bound, max=bound).astype(kind)


def setup_inputs(seed: int = 0) -> dict:
    keys = jax.random.split(jax.random.key(seed), 16)
    residual_in = bell_draw(keys[0], (SEQS, SEQ, D), 1.0, 6.0, ((0, 8), (1, 16)))
    query_proj = draw_query_proj(jax.random.fold_in(keys[15], 71), 0)
    key_proj = draw_key_proj(jax.random.fold_in(keys[15], 71), 0)
    value_proj = bell_draw(keys[3], (SEQS, SEQ, KV_HEADS * HEAD_DIM), 1.0, 6.0, ((0, 8), (1, 16)))
    query_gain = draw_query_gain(jax.random.fold_in(keys[15], 71), 0)
    key_gain = draw_key_gain(jax.random.fold_in(keys[15], 71), 0)
    out_weight = bell_draw(keys[6], (D, D), D ** -0.5, 0.125)
    post_gain = jnp.clip(1.0 + 0.18 * jax.random.normal(keys[7], (D,), jnp.float32), 0.1, 1.9)
    pre_gain = jnp.clip(1.0 + 0.18 * jax.random.normal(keys[8], (D,), jnp.float32), 0.1, 1.9)
    route_ids = draw_route_ids(jax.random.fold_in(keys[15], 71), 0)
    group_weight = jnp.clip(0.25 + 0.75 * jax.random.uniform(keys[10], (SEQS, SEQ), jnp.float32) ** level_of(keys[10], (SEQS, SEQ), ((0, 8), (1, 16)), -0.2, 0.2), 0.25, 1.0)
    first_share = jnp.clip(0.5 + 0.5 * jax.random.uniform(keys[11], (SEQS, SEQ), jnp.float32) ** level_of(keys[11], (SEQS, SEQ), ((0, 8), (1, 16)), -0.2, 0.2), 0.5, 1.0)
    gate_weight = bell_draw(keys[12], (EXPERTS, D, FF), D ** -0.5, 0.125, ((0, 128),))
    up_weight = bell_draw(keys[13], (EXPERTS, D, FF), D ** -0.5, 0.125, ((0, 128),))
    down_weight = bell_draw(keys[14], (EXPERTS, FF, D), FF ** -0.5, 0.25, ((0, 128),))
    return {"residual_in": residual_in, "query_proj": query_proj, "key_proj": key_proj, "value_proj": value_proj, "query_gain": query_gain, "key_gain": key_gain, "out_weight": out_weight, "post_gain": post_gain, "pre_gain": pre_gain, "route_ids": route_ids, "group_weight": group_weight, "first_share": first_share, "gate_weight": gate_weight, "up_weight": up_weight, "down_weight": down_weight}


EPSILON = 1e-06

def rotate_heads(raw_heads, gain_vec, positions):
    floats = raw_heads.astype(jnp.float32)
    normed = floats * lax.rsqrt(lax.optimization_barrier(jnp.mean(floats * floats, axis=-1, keepdims=True)) + EPSILON) * gain_vec
    quarter = raw_heads.shape[-1] // 4
    inverse = 10000.0 ** (-jnp.arange(quarter, dtype=jnp.float32) / quarter)
    grid_rows = (positions // GRID_W).astype(jnp.float32)[:, None] * inverse
    grid_cols = (positions % GRID_W).astype(jnp.float32)[:, None] * inverse
    angles = jnp.concatenate([grid_rows, grid_rows, grid_cols, grid_cols], axis=-1)[:, None, :]
    pieces = normed.reshape(normed.shape[:-1] + (2, 2, quarter))
    turned = jnp.stack([-pieces[..., 1, :], pieces[..., 0, :]], axis=-2).reshape(normed.shape)
    return (normed * jnp.cos(angles) + turned * jnp.sin(angles)).astype(jnp.bfloat16)

def attend_blocks(queries, keys_all, values_all):
    count_q, kv_count, group_size, head_width = queries.shape
    block = min(512, count_q)
    blocks = count_q // block
    scale = head_width ** (-0.5)
    zero_index = jnp.zeros((), jnp.int32)

    def one_item(item):
        which = (item // kv_count).astype(jnp.int32)
        head_index = (item % kv_count).astype(jnp.int32)
        start_row = (which * block).astype(jnp.int32)
        q_block = lax.dynamic_slice(queries, (start_row, head_index, zero_index, zero_index), (block, 1, group_size, head_width))[:, 0]
        key_block = lax.dynamic_slice(keys_all, (zero_index, head_index, zero_index), (keys_all.shape[0], 1, head_width))[:, 0]
        value_block = lax.dynamic_slice(values_all, (zero_index, head_index, zero_index), (values_all.shape[0], 1, head_width))[:, 0]
        scores = jnp.einsum('qgd,sd->gqs', q_block.astype(jnp.float32), key_block.astype(jnp.float32)) * scale
        shifted = jnp.exp(scores - lax.optimization_barrier(jnp.max(scores, axis=-1, keepdims=True)))
        weights = (shifted / lax.optimization_barrier(jnp.sum(shifted, axis=-1, keepdims=True))).astype(jnp.bfloat16)
        return jnp.einsum('gqs,sd->qgd', weights.astype(jnp.float32), value_block.astype(jnp.float32)).astype(jnp.bfloat16)
    results = lax.map(one_item, jnp.arange(blocks * kv_count, dtype=jnp.int32))
    results = results.reshape(blocks, kv_count, block, group_size, head_width).transpose(0, 2, 1, 3, 4)
    return results.reshape(count_q, kv_count * group_size * head_width)

def rms_scale(values, gain_vec):
    floats = values.astype(jnp.float32)
    return floats * lax.rsqrt(lax.optimization_barrier(jnp.mean(floats * floats, axis=-1, keepdims=True)) + EPSILON) * gain_vec

def reference(residual_in, query_proj, key_proj, value_proj, query_gain, key_gain, out_weight, post_gain, pre_gain, route_ids, group_weight, first_share, gate_weight, up_weight, down_weight):
    group_size = HEADS // KV_HEADS

    def one_sequence(inputs):
        query_seq, key_seq, value_seq = inputs
        positions = jnp.arange(SEQ, dtype=jnp.int32)
        query_turned = rotate_heads(query_seq.reshape(SEQ, HEADS, HEAD_DIM), query_gain, positions)
        key_turned = rotate_heads(key_seq.reshape(SEQ, KV_HEADS, HEAD_DIM), key_gain, positions)
        return attend_blocks(query_turned.reshape(SEQ, KV_HEADS, group_size, HEAD_DIM), key_turned, value_seq.reshape(SEQ, KV_HEADS, HEAD_DIM))
    attended = lax.map(one_sequence, (query_proj, key_proj, value_proj)).reshape(SEQS * SEQ, D)
    mixed = jnp.dot(attended, out_weight, preferred_element_type=jnp.float32).astype(jnp.bfloat16)
    stream = (residual_in.reshape(SEQS * SEQ, D).astype(jnp.float32) + rms_scale(mixed, post_gain)).astype(jnp.bfloat16)
    normed = rms_scale(stream, pre_gain).astype(jnp.bfloat16)
    chosen = route_ids.reshape(-1).astype(jnp.int32)
    assigns = chosen.shape[0]
    order = jnp.argsort(chosen, stable=True).astype(jnp.int32)
    counts = jax.ops.segment_sum(jnp.ones((assigns,), jnp.int32), chosen, num_segments=EXPERTS).astype(jnp.int32)
    starts = (jnp.cumsum(counts) - counts).astype(jnp.int32)
    most = CAP * N_SP * N_DP
    order_pad = jnp.concatenate([order, jnp.full((most,), assigns, jnp.int32)])
    normed_pad = jnp.concatenate([normed, jnp.zeros((1, D), jnp.bfloat16)], axis=0)

    def per_expert(carry, inputs):
        index, gate_one, up_one, down_one = inputs
        picked = lax.dynamic_slice(order_pad, (starts[index].astype(jnp.int32),), (most,))
        valid = jnp.arange(most, dtype=jnp.int32) < counts[index]
        picked = jnp.where(valid, picked, assigns).astype(jnp.int32)
        rows_in = normed_pad[picked // 2]
        gated = jnp.dot(rows_in, gate_one, preferred_element_type=jnp.float32)
        lifted = jnp.dot(rows_in, up_one, preferred_element_type=jnp.float32)
        hidden = (jax.nn.silu(gated) * lifted).astype(jnp.bfloat16)
        produced = jnp.dot(hidden, down_one, preferred_element_type=jnp.float32).astype(jnp.bfloat16)
        return (carry.at[picked].set(produced), None)
    outputs, _ = lax.scan(per_expert, jnp.zeros((assigns + 1, D), jnp.bfloat16), (jnp.arange(EXPERTS, dtype=jnp.int32), gate_weight, up_weight, down_weight))
    results = outputs[:assigns].astype(jnp.float32).reshape(SEQS * SEQ, 2, D)
    share = first_share.reshape(-1)
    weight_pair = group_weight.reshape(-1)[:, None] * jnp.stack([share, 1.0 - share], axis=1)
    combined = lax.optimization_barrier(jnp.sum(weight_pair[:, :, None] * results, axis=1))
    return (stream.astype(jnp.float32) + combined).astype(jnp.bfloat16).reshape(SEQS, SEQ, D)
```

```python
import functools

import jax
import jax.numpy as jnp
import numpy as np
from jax import lax
from jax.experimental import pallas as pl
from jax.experimental.pallas import tpu as pltpu
from jax.sharding import Mesh
from jax.sharding import PartitionSpec as P

HEADS = 16
KV_HEADS = 4
HEAD_DIM = 128
GRID_W = 64
CAP = 4
EPSILON = 1e-06
F32 = jnp.float32
BF16 = jnp.bfloat16


def dot(a, b, dims=((1,), (0,))):
    return lax.dot_general(a, b, (dims, ((), ())), preferred_element_type=F32)


def pack_kernel(place_ref, q_ref, k_ref, v_ref, qg_ref, kg_ref, inv_ref, out_ref, cos_ref, sin_ref):
    tokens = k_ref.shape[0]
    shape = (tokens, HEAD_DIM)
    lane = lax.broadcasted_iota(jnp.int32, shape, 1)
    first = lax.bitwise_and(lane, 32) == 0

    @pl.when(pl.program_id(0) == 0)
    def _():
        position = place_ref[0] * tokens + lax.broadcasted_iota(jnp.int32, shape, 0)
        grid_row = lax.shift_right_logical(position, 6)
        grid_col = lax.bitwise_and(position, GRID_W - 1)
        angles = jnp.where(lane < HEAD_DIM // 2, grid_row, grid_col).astype(F32) * inv_ref[...]
        sin = jnp.sin(angles)
        cos_ref[...] = jnp.cos(angles)
        sin_ref[...] = jnp.where(first, -sin, sin)

    cos = cos_ref[...]
    sin = sin_ref[...]

    def turned(raw, gain):
        floats = raw.astype(F32)
        mean = jnp.mean(floats * floats, axis=-1, keepdims=True)
        normed = floats * lax.rsqrt(mean + EPSILON) * gain
        other = jnp.where(first, pltpu.roll(normed, 96, 1), pltpu.roll(normed, 32, 1))
        return (normed * cos + other * sin).astype(BF16)

    key = turned(k_ref[...], kg_ref[...])
    value = v_ref[...]
    for h in range(out_ref.shape[0]):
        query = turned(q_ref[:, h * HEAD_DIM : (h + 1) * HEAD_DIM], qg_ref[...])
        out_ref[h, :, 0:HEAD_DIM] = query
        out_ref[h, :, HEAD_DIM : 2 * HEAD_DIM] = key
        out_ref[h, :, 2 * HEAD_DIM : 3 * HEAD_DIM] = value


def attend_kernel(x_ref, out_ref, value_ref, even_ref, odd_ref):
    length = x_ref.shape[0]
    block = even_ref.shape[0]
    blocks = length // block
    value_ref[:, 0:HEAD_DIM] = x_ref[:, 2 * HEAD_DIM : 3 * HEAD_DIM]
    value_ref[:, HEAD_DIM:] = jnp.ones((length, HEAD_DIM), BF16)
    scale = float(HEAD_DIM ** (-0.5) * np.log2(np.e))

    def score(i, score_ref):
        rows = pl.ds(pl.multiple_of(i * block, block), block)
        score_ref[...] = dot(x_ref[rows, 0:HEAD_DIM], x_ref[:, HEAD_DIM : 2 * HEAD_DIM], ((1,), (1,)))

    def mix(i, score_ref):
        rows = pl.ds(pl.multiple_of(i * block, block), block)
        top = jnp.max(score_ref[...], axis=-1, keepdims=True)
        weights = jnp.exp2((score_ref[...] - top) * scale).astype(BF16)
        both = dot(weights, value_ref[...])
        out_ref[rows, :] = (both[:, 0:HEAD_DIM] / both[:, HEAD_DIM:]).astype(BF16)

    score(0, even_ref)

    def two(j, carry):
        i = 2 * j
        score(i + 1, odd_ref)
        mix(i, even_ref)
        score(jnp.minimum(i + 2, blocks - 1), even_ref)
        mix(i + 1, odd_ref)
        return carry

    lax.fori_loop(0, blocks // 2, two, 0)


def rms(floats, gain):
    return floats * lax.rsqrt(jnp.mean(floats * floats, axis=-1, keepdims=True) + EPSILON) * gain


def proj_kernel(place_ref, att_ref, w_ref, res_ref, post_ref, pre_ref, ids_ref, *rest):
    *_, out_ref, stream_ref, slot_ref, x_ref = rest
    tokens, width = x_ref.shape
    for h in range(HEADS):
        x_ref[:, h * HEAD_DIM : (h + 1) * HEAD_DIM] = att_ref[h]
    experts = 2 * out_ref.shape[0]
    which = lax.broadcasted_iota(jnp.int32, (experts, tokens), 0)
    first = ids_ref[0:1, :]
    second = ids_ref[1:2, :]
    hit_first = jnp.where(which == first, 1.0, 0.0)
    hit_second = jnp.where(which == second, 1.0, 0.0)
    row = lax.broadcasted_iota(jnp.int32, (tokens, tokens), 0)
    col = lax.broadcasted_iota(jnp.int32, (tokens, tokens), 1)
    before = jnp.where(row < col, 1.0, 0.0).astype(BF16)
    rank = dot((hit_first + hit_second).astype(BF16), before)
    rank_first = jnp.sum(rank * hit_first, axis=0, keepdims=True).astype(jnp.int32)
    rank_second = jnp.sum(rank * hit_second, axis=0, keepdims=True).astype(jnp.int32)
    core = place_ref[1]

    def slot_of(expert, rank):
        side = lax.bitwise_xor(lax.bitwise_and(expert, 1), core)
        return lax.shift_right_logical(expert, 1) * (2 * CAP) + rank * 2 + side

    slot_first = slot_of(first, rank_first)
    slot_second = slot_of(second, rank_second)
    slot_ref[0:1, :] = slot_first
    slot_ref[1:2, :] = slot_second
    slot = lax.broadcasted_iota(jnp.int32, (experts * CAP, tokens), 0)
    here = (slot == slot_first) | (slot == slot_second)
    picks = jnp.where(here, 1.0, 0.0).astype(BF16)
    mixed = dot(x_ref[...], w_ref[...]).astype(BF16).astype(F32)
    stream = (res_ref[...].astype(F32) + rms(mixed, post_ref[...])).astype(BF16)
    stream_ref[...] = stream
    normed = rms(stream.astype(F32), pre_ref[...]).astype(BF16)
    out_ref[...] = dot(picks, normed).astype(BF16).reshape(out_ref.shape)


def expert_kernel(y_ref, *rest):
    *weights, out_ref, wide_ref, x_ref = rest
    slots, width = y_ref.shape
    sides = [pl.ds(side, slots // 2, stride=2) for side in range(2)]
    blocks = [slice(c * 128, (c + 1) * 128) for c in range(width // 128)]
    for c, cols in enumerate(blocks):
        wide_ref[c] = y_ref[:, cols].astype(F32)
        for side in range(2):
            x_ref[side, :, cols] = wide_ref[c, sides[side], :].astype(BF16)
    for side in range(2):
        gate_ref, up_ref, down_ref = weights[3 * side : 3 * side + 3]
        gated = dot(x_ref[side], gate_ref[...])
        lifted = dot(x_ref[side], up_ref[...])
        hidden = (gated / (1.0 + jnp.exp(-gated)) * lifted).astype(BF16)
        made = dot(hidden, down_ref[...])
        for c, cols in enumerate(blocks):
            wide_ref[c, sides[side], :] = made[:, cols]
    for c, cols in enumerate(blocks):
        out_ref[:, cols] = wide_ref[c].astype(BF16)


def combine_kernel(z_ref, stream_ref, slot_ref, weight_ref, share_ref, out_ref):
    slots = z_ref.shape[0]
    tokens, width = stream_ref.shape
    slot = lax.broadcasted_iota(jnp.int32, (slots, tokens), 0)
    picks = [jnp.where(slot == slot_ref[i : i + 1, :], 1.0, 0.0).astype(BF16) for i in range(2)]
    picked = dot(jnp.concatenate(picks, axis=1), z_ref[...], ((0,), (0,)))
    column = lambda row: jnp.broadcast_to(row, (tokens, tokens)).T[:, 0:1]
    weight = weight_ref[...]
    share = share_ref[...]
    weight_first = column(weight * share)
    weight_second = column(weight * (1.0 - share))
    ffn = weight_first * picked[0:tokens] + weight_second * picked[tokens:]
    out_ref[...] = (stream_ref[...].astype(F32) + ffn).astype(BF16)


def local(
    residual_in,
    query_proj,
    key_proj,
    value_proj,
    query_gain,
    key_gain,
    out_weight,
    post_gain,
    pre_gain,
    route_ids,
    group_weight,
    first_share,
    gate_weight,
    up_weight,
    down_weight,
):
    sp_count = lax.axis_size("sp")
    tokens, width = query_proj.shape[1:]
    length = tokens * sp_count
    chips = sp_count * lax.axis_size("y")
    experts = 2 * chips
    assert sp_count == HEADS and gate_weight.shape[0] == 1 and lax.axis_size("core") == 2
    quarter = HEAD_DIM // 4
    inverse = np.float32(10000.0) ** (-np.arange(quarter, dtype=np.float32) / np.float32(quarter))
    inverse = jnp.asarray(np.tile(inverse.astype(np.float32), 4)[None])
    place = jnp.stack([lax.axis_index("sp"), lax.axis_index("core")]).astype(jnp.int32)
    swap = [(0, 1), (1, 0)]
    own = (gate_weight[0], up_weight[0], down_weight[0])
    partner = tuple(lax.ppermute(one, "core", swap) for one in own)

    vmem = pl.BlockSpec(memory_space=pltpu.VMEM)
    smem = pl.BlockSpec(memory_space=pltpu.SMEM)
    limit = lambda mib: pltpu.CompilerParams(vmem_limit_bytes=mib * 2**20)
    group = HEADS // KV_HEADS
    fixed = lambda *shape: pl.BlockSpec(shape, lambda n: (0,) * len(shape))
    packed = pl.pallas_call(
        pack_kernel,
        grid=(KV_HEADS,),
        out_shape=jax.ShapeDtypeStruct((HEADS, tokens, 3 * HEAD_DIM), BF16),
        in_specs=[
            smem,
            pl.BlockSpec((tokens, group * HEAD_DIM), lambda n: (0, n)),
            pl.BlockSpec((tokens, HEAD_DIM), lambda n: (0, n)),
            pl.BlockSpec((tokens, HEAD_DIM), lambda n: (0, n)),
            fixed(1, HEAD_DIM),
            fixed(1, HEAD_DIM),
            fixed(1, HEAD_DIM),
        ],
        out_specs=pl.BlockSpec((group, tokens, 3 * HEAD_DIM), lambda n: (n, 0, 0)),
        scratch_shapes=[pltpu.VMEM((tokens, HEAD_DIM), F32)] * 2,
        compiler_params=limit(63),
        name="pack",
    )(place, query_proj[0], key_proj[0], value_proj[0], query_gain[None], key_gain[None], inverse)
    gathered = lax.all_to_all(packed, "sp", 0, 0, tiled=True)
    block = 512
    attended = pl.pallas_call(
        attend_kernel,
        out_shape=jax.ShapeDtypeStruct((length, HEAD_DIM), BF16),
        in_specs=[vmem],
        out_specs=vmem,
        scratch_shapes=[
            pltpu.VMEM((length, 2 * HEAD_DIM), BF16),
            pltpu.VMEM((block, length), F32),
            pltpu.VMEM((block, length), F32),
        ],
        compiler_params=limit(24),
        cost_estimate=pl.CostEstimate(
            flops=4 * length * length * HEAD_DIM * 4,
            bytes_accessed=length * HEAD_DIM * 8,
            transcendentals=length * length,
        ),
        name="attend",
    )(gathered.reshape(length, 3 * HEAD_DIM))
    attended = lax.all_to_all(attended.reshape(sp_count, tokens, HEAD_DIM), "sp", 0, 0, tiled=True)
    hbm = pl.BlockSpec(memory_space=pltpu.HBM)
    sent, stream, slots = pl.pallas_call(
        proj_kernel,
        out_shape=(
            jax.ShapeDtypeStruct((chips, 2 * CAP, width), BF16),
            jax.ShapeDtypeStruct((tokens, width), BF16),
            jax.ShapeDtypeStruct((8, tokens), jnp.int32),
        ),
        in_specs=[smem] + [vmem] * 6 + [hbm] * 3,
        out_specs=(vmem,) * 3,
        scratch_shapes=[
            pltpu.VMEM((tokens, width), BF16),
        ],
        compiler_params=limit(24),
        name="project",
    )(
        place,
        attended,
        out_weight,
        residual_in[0],
        post_gain[None],
        pre_gain[None],
        route_ids[0].T,
        *partner,
    )
    peers = ("sp", "y")
    arrived = lax.all_to_all(sent, peers, 0, 0, tiled=True)
    rows = experts * CAP
    answered = pl.pallas_call(
        expert_kernel,
        out_shape=jax.ShapeDtypeStruct((rows, width), BF16),
        in_specs=[vmem] * 7,
        out_specs=vmem,
        scratch_shapes=[
            pltpu.VMEM((width // 128, rows, 128), F32),
            pltpu.VMEM((2, rows // 2, width), BF16),
        ],
        compiler_params=limit(24),
        name="expert",
    )(arrived.reshape(rows, width), *own, *partner)
    returned = lax.all_to_all(answered.reshape(chips, 2 * CAP, width), peers, 0, 0, tiled=True)
    combined = pl.pallas_call(
        combine_kernel,
        out_shape=jax.ShapeDtypeStruct((tokens, width), BF16),
        in_specs=[vmem] * 5,
        out_specs=vmem,
        compiler_params=limit(16),
        name="combine",
    )(returned.reshape(rows, width), stream, slots, group_weight, first_share)
    return combined[None]


def solution(mesh):
    assert mesh.axis_names[0] == "sp"
    grid = mesh.devices.reshape(mesh.devices.shape[0], -1, 2)
    mesh = Mesh(grid, ("sp", "y", "core"))
    placed = (
        P(("y", "core"), "sp", None),
        P(("y", "core"), "sp", None),
        P(("y", "core"), "sp", None),
        P(("y", "core"), "sp", None),
        P(),
        P(),
        P(),
        P(),
        P(),
        P(("y", "core"), "sp", None),
        P(("y", "core"), "sp"),
        P(("y", "core"), "sp"),
        P(("sp", "y", "core"), None, None),
        P(("sp", "y", "core"), None, None),
        P(("sp", "y", "core"), None, None),
    )
    return jax.shard_map(
        local, mesh=mesh, in_specs=placed, out_specs=P(("y", "core"), "sp", None), check_vma=False
    )
```

```python
import functools

import jax
import jax.numpy as jnp
import numpy as np
from jax import lax
from jax.experimental import pallas as pl
from jax.experimental.pallas import tpu as pltpu
from jax.sharding import Mesh
from jax.sharding import PartitionSpec as P

HEADS = 16
KV_HEADS = 4
HEAD_DIM = 128
GRID_W = 64
CAP = 4
EPSILON = 1e-06
F32 = jnp.float32
BF16 = jnp.bfloat16


def dot(a, b, dims=((1,), (0,))):
    return lax.dot_general(a, b, (dims, ((), ())), preferred_element_type=F32)


def angle_tables(count):
    quarter = HEAD_DIM // 4
    inverse = np.float32(10000.0) ** (-np.arange(quarter, dtype=np.float32) / np.float32(quarter))
    angles = np.arange(count, dtype=np.float32)[:, None] * inverse.astype(np.float32)
    angles = np.tile(angles.astype(np.float64), (1, 4))
    return np.stack([np.cos(angles), np.sin(angles)]).astype(np.float32)


def partner_matrix():
    lane = np.arange(HEAD_DIM)
    low = (lane & 32) == 0
    matrix = np.zeros((HEAD_DIM, HEAD_DIM), np.float32)
    matrix[np.where(low, lane + 32, lane - 32), lane] = np.where(low, -1.0, 1.0)
    return matrix


def pack_kernel(
    place_ref, q_ref, k_ref, v_ref, qg_ref, kg_ref, row_ref, col_ref, swap_ref, out_ref, table_ref
):
    tokens = k_ref.shape[0]
    group = out_ref.shape[0]

    @pl.when(pl.program_id(0) == 0)
    def _():
        lane = lax.broadcasted_iota(jnp.int32, (GRID_W, HEAD_DIM), 1)
        line = lax.broadcasted_iota(jnp.int32, (1, HEAD_DIM), 1)
        low = lax.bitwise_and(line, 32) == 0
        start = lax.shift_right_logical(place_ref[0], 3) * (tokens // GRID_W)
        for which, gain_ref in enumerate((qg_ref, kg_ref)):
            gain = gain_ref[...]
            wide = jnp.broadcast_to(gain, (8, HEAD_DIM))
            other = jnp.where(low, pltpu.roll(wide, 96, 1)[0:1], pltpu.roll(wide, 32, 1)[0:1])
            for kind, scale in enumerate((gain, other)):
                for i in range(tokens // GRID_W):
                    at_row = row_ref[kind, pl.ds(start + i, 1), :]
                    table = jnp.where(lane < HEAD_DIM // 2, at_row, col_ref[kind])
                    table_ref[which, kind, i * GRID_W : (i + 1) * GRID_W, :] = table * scale

    ones = jnp.ones((HEAD_DIM, HEAD_DIM), BF16)
    raw = [q_ref[:, h * HEAD_DIM : (h + 1) * HEAD_DIM] for h in range(group)] + [k_ref[...]]
    raw = jnp.concatenate(raw, axis=0)
    floats = raw.astype(F32)
    square = floats * floats
    high = square.astype(BF16)
    low_part = (square - high.astype(F32)).astype(BF16)
    total = dot(high, ones) + dot(low_part, ones)
    scale = lax.rsqrt(total * (1.0 / HEAD_DIM) + EPSILON)
    other = dot(raw, swap_ref[...])
    value = v_ref[...]
    for h in range(group, -1, -1):
        rows = slice(h * tokens, (h + 1) * tokens)
        which = 1 if h == group else 0
        turned = floats[rows] * table_ref[which, 0] + other[rows] * table_ref[which, 1]
        turned = (turned * scale[rows]).astype(BF16)
        if h == group:
            for g in range(group):
                out_ref[g, :, HEAD_DIM : 2 * HEAD_DIM] = turned
                out_ref[g, :, 2 * HEAD_DIM : 3 * HEAD_DIM] = value
        else:
            out_ref[h, :, 0:HEAD_DIM] = turned


def attend_kernel(x_ref, out_ref, value_ref, even_ref, odd_ref):
    length = x_ref.shape[0]
    block = even_ref.shape[0]
    blocks = length // block
    value_ref[:, 0:HEAD_DIM] = x_ref[:, 2 * HEAD_DIM : 3 * HEAD_DIM]
    value_ref[:, HEAD_DIM:] = jnp.ones((length, HEAD_DIM), BF16)
    scale = float(HEAD_DIM ** (-0.5) * np.log2(np.e))

    def score(i, score_ref):
        rows = pl.ds(pl.multiple_of(i * block, block), block)
        score_ref[...] = dot(x_ref[rows, 0:HEAD_DIM], x_ref[:, HEAD_DIM : 2 * HEAD_DIM], ((1,), (1,)))

    def mix(i, score_ref):
        rows = pl.ds(pl.multiple_of(i * block, block), block)
        top = jnp.max(score_ref[...], axis=-1, keepdims=True)
        weights = jnp.exp2((score_ref[...] - top) * scale).astype(BF16)
        both = dot(weights, value_ref[...])
        out_ref[rows, :] = (both[:, 0:HEAD_DIM] / both[:, HEAD_DIM:]).astype(BF16)

    score(0, even_ref)

    def two(j, carry):
        i = 2 * j
        score(i + 1, odd_ref)
        mix(i, even_ref)
        score(jnp.minimum(i + 2, blocks - 1), even_ref)
        mix(i + 1, odd_ref)
        return carry

    lax.fori_loop(0, blocks // 2, two, 0)


def rms(floats, gain):
    return floats * lax.rsqrt(jnp.mean(floats * floats, axis=-1, keepdims=True) + EPSILON) * gain


def proj_kernel(place_ref, att_ref, w_ref, res_ref, post_ref, pre_ref, ids_ref, *rest):
    *_, out_ref, stream_ref, slot_ref, x_ref = rest
    tokens, width = x_ref.shape
    for h in range(HEADS):
        x_ref[:, h * HEAD_DIM : (h + 1) * HEAD_DIM] = att_ref[h]
    experts = 2 * out_ref.shape[0]
    which = lax.broadcasted_iota(jnp.int32, (experts, tokens), 0)
    first = ids_ref[0:1, :]
    second = ids_ref[1:2, :]
    hit_first = jnp.where(which == first, 1.0, 0.0)
    hit_second = jnp.where(which == second, 1.0, 0.0)
    row = lax.broadcasted_iota(jnp.int32, (tokens, tokens), 0)
    col = lax.broadcasted_iota(jnp.int32, (tokens, tokens), 1)
    before = jnp.where(row < col, 1.0, 0.0).astype(BF16)
    rank = dot((hit_first + hit_second).astype(BF16), before)
    rank_first = jnp.sum(rank * hit_first, axis=0, keepdims=True).astype(jnp.int32)
    rank_second = jnp.sum(rank * hit_second, axis=0, keepdims=True).astype(jnp.int32)
    core = lax.bitwise_and(place_ref[0], 1)

    def slot_of(expert, rank):
        side = lax.bitwise_xor(lax.bitwise_and(expert, 1), core)
        return lax.shift_right_logical(expert, 1) * (2 * CAP) + rank * 2 + side

    slot_first = slot_of(first, rank_first)
    slot_second = slot_of(second, rank_second)
    slot_ref[0:1, :] = slot_first
    slot_ref[1:2, :] = slot_second
    slot = lax.broadcasted_iota(jnp.int32, (experts * CAP, tokens), 0)
    here = (slot == slot_first) | (slot == slot_second)
    picks = jnp.where(here, 1.0, 0.0).astype(BF16)
    mixed = dot(x_ref[...], w_ref[...]).astype(BF16).astype(F32)
    stream = (res_ref[...].astype(F32) + rms(mixed, post_ref[...])).astype(BF16)
    stream_ref[...] = stream
    normed = rms(stream.astype(F32), pre_ref[...]).astype(BF16)
    out_ref[...] = dot(picks, normed).astype(BF16).reshape(out_ref.shape)


def expert_kernel(y_ref, *rest):
    weights, late, (out_ref, wide_ref, x_ref, *held, sems) = list(rest[:4]), rest[4:6], rest[6:]
    copies = [pltpu.make_async_copy(late[i], held[i], sems.at[i]) for i in range(2)]
    for copy in copies:
        copy.start()
    weights += held
    slots, width = y_ref.shape
    sides = [pl.ds(side, slots // 2, stride=2) for side in range(2)]
    blocks = [slice(c * 128, (c + 1) * 128) for c in range(width // 128)]
    for c, cols in enumerate(blocks):
        wide_ref[c] = y_ref[:, cols].astype(F32)
        for side in range(2):
            x_ref[side, :, cols] = wide_ref[c, sides[side], :].astype(BF16)
    for side in range(2):
        gate_ref, up_ref, down_ref = weights[3 * side : 3 * side + 3]
        gated = dot(x_ref[side], gate_ref[...])
        if side == 1:
            copies[0].wait()
        lifted = dot(x_ref[side], up_ref[...])
        hidden = (gated / (1.0 + jnp.exp(-gated)) * lifted).astype(BF16)
        if side == 1:
            copies[1].wait()
        made = dot(hidden, down_ref[...])
        for c, cols in enumerate(blocks):
            wide_ref[c, sides[side], :] = made[:, cols]
    for c, cols in enumerate(blocks):
        out_ref[:, cols] = wide_ref[c].astype(BF16)


def combine_kernel(z_ref, stream_ref, slot_ref, weight_ref, share_ref, out_ref):
    slots = z_ref.shape[0]
    tokens, width = stream_ref.shape
    slot = lax.broadcasted_iota(jnp.int32, (slots, tokens), 0)
    picks = [jnp.where(slot == slot_ref[i : i + 1, :], 1.0, 0.0).astype(BF16) for i in range(2)]
    picked = dot(jnp.concatenate(picks, axis=1), z_ref[...], ((0,), (0,)))
    column = lambda row: jnp.broadcast_to(row, (tokens, tokens)).T[:, 0:1]
    weight = weight_ref[...]
    share = share_ref[...]
    weight_first = column(weight * share)
    weight_second = column(weight * (1.0 - share))
    ffn = weight_first * picked[0:tokens] + weight_second * picked[tokens:]
    out_ref[...] = (stream_ref[...].astype(F32) + ffn).astype(BF16)


def local(
    residual_in,
    query_proj,
    key_proj,
    value_proj,
    query_gain,
    key_gain,
    out_weight,
    post_gain,
    pre_gain,
    route_ids,
    group_weight,
    first_share,
    gate_weight,
    up_weight,
    down_weight,
):
    line = ("x", "z")
    sp_count = lax.axis_size(line)
    tokens, width = query_proj.shape[1:]
    length = tokens * sp_count
    chips = sp_count * lax.axis_size("y")
    experts = 2 * chips
    assert sp_count == HEADS and gate_weight.shape[0] == 1 and lax.axis_size("core") == 2
    place = lax.axis_index(("z", "x", "y", "core")).astype(jnp.int32).reshape(1)
    row_table = jnp.asarray(angle_tables(length // GRID_W))
    col_table = jnp.asarray(angle_tables(GRID_W))
    swap_table = jnp.asarray(partner_matrix(), BF16)
    swap = [(0, 1), (1, 0)]
    own = (gate_weight[0], up_weight[0], down_weight[0])
    partner = tuple(lax.ppermute(one, "core", swap) for one in own)

    vmem = pl.BlockSpec(memory_space=pltpu.VMEM)
    smem = pl.BlockSpec(memory_space=pltpu.SMEM)
    limit = lambda mib: pltpu.CompilerParams(vmem_limit_bytes=mib * 2**20)
    group = HEADS // KV_HEADS
    fixed = lambda *shape: pl.BlockSpec(shape, lambda n: (0,) * len(shape))
    packed = pl.pallas_call(
        pack_kernel,
        grid=(KV_HEADS,),
        out_shape=jax.ShapeDtypeStruct((HEADS, tokens, 3 * HEAD_DIM), BF16),
        in_specs=[
            smem,
            pl.BlockSpec((tokens, group * HEAD_DIM), lambda n: (0, n)),
            pl.BlockSpec((tokens, HEAD_DIM), lambda n: (0, n)),
            pl.BlockSpec((tokens, HEAD_DIM), lambda n: (0, n)),
            fixed(1, HEAD_DIM),
            fixed(1, HEAD_DIM),
            fixed(*row_table.shape),
            fixed(*col_table.shape),
            fixed(*swap_table.shape),
        ],
        out_specs=pl.BlockSpec((group, tokens, 3 * HEAD_DIM), lambda n: (n, 0, 0)),
        scratch_shapes=[pltpu.VMEM((2, 2, tokens, HEAD_DIM), F32)],
        compiler_params=limit(63),
        name="pack",
    )(
        place,
        query_proj[0],
        key_proj[0],
        value_proj[0],
        query_gain[None],
        key_gain[None],
        row_table,
        col_table,
        swap_table,
    )
    gathered = lax.all_to_all(packed, line, 0, 0, tiled=True)
    block = 512
    attended = pl.pallas_call(
        attend_kernel,
        out_shape=jax.ShapeDtypeStruct((length, HEAD_DIM), BF16),
        in_specs=[vmem],
        out_specs=vmem,
        scratch_shapes=[
            pltpu.VMEM((length, 2 * HEAD_DIM), BF16),
            pltpu.VMEM((block, length), F32),
            pltpu.VMEM((block, length), F32),
        ],
        compiler_params=limit(24),
        cost_estimate=pl.CostEstimate(
            flops=4 * length * length * HEAD_DIM * 4,
            bytes_accessed=length * HEAD_DIM * 8,
            transcendentals=length * length,
        ),
        name="attend",
    )(gathered.reshape(length, 3 * HEAD_DIM))
    attended = lax.all_to_all(attended.reshape(sp_count, tokens, HEAD_DIM), line, 0, 0, tiled=True)
    hbm = pl.BlockSpec(memory_space=pltpu.HBM)
    sent, stream, slots = pl.pallas_call(
        proj_kernel,
        out_shape=(
            jax.ShapeDtypeStruct((chips, 2 * CAP, width), BF16),
            jax.ShapeDtypeStruct((tokens, width), BF16),
            jax.ShapeDtypeStruct((8, tokens), jnp.int32),
        ),
        in_specs=[smem] + [vmem] * 6 + [hbm] * 3,
        out_specs=(vmem,) * 3,
        scratch_shapes=[
            pltpu.VMEM((tokens, width), BF16),
        ],
        compiler_params=limit(24),
        name="project",
    )(
        place,
        attended,
        out_weight,
        residual_in[0],
        post_gain[None],
        pre_gain[None],
        route_ids[0].T,
        *partner,
    )
    peers = ("z", "x", "y")
    arrived = lax.all_to_all(sent, peers, 0, 0, tiled=True)
    rows = experts * CAP
    answered = pl.pallas_call(
        expert_kernel,
        out_shape=jax.ShapeDtypeStruct((rows, width), BF16),
        in_specs=[vmem] * 5 + [hbm] * 2,
        out_specs=vmem,
        scratch_shapes=[
            pltpu.VMEM((width // 128, rows, 128), F32),
            pltpu.VMEM((2, rows // 2, width), BF16),
            *[pltpu.VMEM(one.shape, BF16) for one in partner[1:]],
            pltpu.SemaphoreType.DMA((2,)),
        ],
        compiler_params=limit(24),
        name="expert",
    )(arrived.reshape(rows, width), *own, *partner)
    returned = lax.all_to_all(answered.reshape(chips, 2 * CAP, width), peers, 0, 0, tiled=True)
    combined = pl.pallas_call(
        combine_kernel,
        out_shape=jax.ShapeDtypeStruct((tokens, width), BF16),
        in_specs=[vmem] * 5,
        out_specs=vmem,
        compiler_params=limit(16),
        name="combine",
    )(returned.reshape(rows, width), stream, slots, group_weight, first_share)
    return combined[None]


def solution(mesh):
    assert mesh.devices.shape == (16, 8)
    grid = mesh.devices.reshape(4, 4, 4, 2)
    mesh = Mesh(grid, ("z", "x", "y", "core"))
    placed = (
        P(("y", "core"), ("z", "x"), None),
        P(("y", "core"), ("z", "x"), None),
        P(("y", "core"), ("z", "x"), None),
        P(("y", "core"), ("z", "x"), None),
        P(),
        P(),
        P(),
        P(),
        P(),
        P(("y", "core"), ("z", "x"), None),
        P(("y", "core"), ("z", "x")),
        P(("y", "core"), ("z", "x")),
        P(("z", "x", "y", "core"), None, None),
        P(("z", "x", "y", "core"), None, None),
        P(("z", "x", "y", "core"), None, None),
    )
    return jax.shard_map(
        local, mesh=mesh, in_specs=placed, out_specs=P(("y", "core"), ("z", "x"), None), check_vma=False
    )
```

```python
import functools

import jax
import jax.numpy as jnp
import numpy as np
from jax import lax
from jax.experimental import pallas as pl
from jax.experimental.pallas import tpu as pltpu
from jax.sharding import Mesh
from jax.sharding import PartitionSpec as P

HEADS = 16
KV_HEADS = 4
HEAD_DIM = 128
GRID_W = 64
GROUP_BITS = 5
CAP = 4
EPSILON = 1e-06
F32 = jnp.float32
BF16 = jnp.bfloat16


def dot(a, b, dims=((1,), (0,))):
    return lax.dot_general(a, b, (dims, ((), ())), preferred_element_type=F32)


def angle_tables(count):
    quarter = HEAD_DIM // 4
    inverse = np.float32(10000.0) ** (-np.arange(quarter, dtype=np.float32) / np.float32(quarter))
    angles = np.arange(count, dtype=np.float32)[:, None] * inverse.astype(np.float32)
    angles = np.tile(angles.astype(np.float64), (1, 4))
    return np.stack([np.cos(angles), np.sin(angles)]).astype(np.float32)


def partner_matrix():
    lane = np.arange(HEAD_DIM)
    low = (lane & 32) == 0
    matrix = np.zeros((HEAD_DIM, HEAD_DIM), np.float32)
    matrix[np.where(low, lane + 32, lane - 32), lane] = np.where(low, -1.0, 1.0)
    return matrix


def earlier(tokens, block):
    row = lax.broadcasted_iota(jnp.int32, (tokens, tokens), 0)
    col = lax.broadcasted_iota(jnp.int32, (tokens, tokens), 1)
    same = lax.shift_right_logical(row, block) == lax.shift_right_logical(col, block)
    return jnp.where((row < col) & same, 1.0, 0.0).astype(BF16)


def group_positions(ids_ref):
    tokens = ids_ref.shape[1]
    group = lax.shift_right_logical(ids_ref[0:1, :], GROUP_BITS)
    hit = jnp.where(lax.broadcasted_iota(jnp.int32, (8, tokens), 0) == group, 1.0, 0.0)
    rank = dot(hit.astype(BF16), earlier(tokens, 31))
    rank = jnp.sum(rank * hit, axis=0, keepdims=True).astype(jnp.int32)
    return group * (tokens // 4) + rank


def three_pieces(row):
    high = row.astype(BF16).astype(F32)
    middle = (row - high).astype(BF16).astype(F32)
    return [high, middle, row - high - middle]


def pack_kernel(
    place_ref,
    q_ref,
    k_ref,
    v_ref,
    res_ref,
    qg_ref,
    kg_ref,
    row_ref,
    col_ref,
    swap_ref,
    ids_ref,
    weight_ref,
    share_ref,
    out_ref,
    *rest,
):
    *block_refs, table_ref, sort_ref, shift_ref = rest
    tokens = k_ref.shape[0]
    group = out_ref.shape[0]
    width = 4 * res_ref.shape[1]

    @pl.when(pl.program_id(0) == 0)
    def _():
        position = group_positions(ids_ref)
        row = lax.broadcasted_iota(jnp.int32, (tokens, tokens), 0)
        sort_ref[...] = jnp.where(row == position, 1.0, 0.0).astype(BF16)
        plane = lax.shift_right_logical(place_ref[0], 5)
        target = lax.bitwise_and(lax.shift_right_logical(row, 5) + plane, 3) * 32
        target = target + lax.bitwise_and(row, 31)
        shifted = jnp.where(target == position, 1.0, 0.0).astype(BF16)
        shift_ref[...] = shifted
        facts = [ids_ref[0:1, :].astype(F32), ids_ref[1:2, :].astype(F32)]
        facts += three_pieces(weight_ref[...]) + three_pieces(share_ref[...])
        facts.append(jnp.zeros((tokens - len(facts), tokens), F32))
        facts = dot(shifted, jnp.concatenate(facts, axis=0).astype(BF16), ((1,), (1,))).astype(BF16)
        for i, block_ref in enumerate(block_refs):
            block_ref[:, width:] = facts[32 * i : 32 * (i + 1)]

    @pl.when(pl.program_id(0) == 0)
    def _():
        lane = lax.broadcasted_iota(jnp.int32, (GRID_W, HEAD_DIM), 1)
        line = lax.broadcasted_iota(jnp.int32, (1, HEAD_DIM), 1)
        low = lax.bitwise_and(line, 32) == 0
        start = lax.shift_right_logical(place_ref[0], 3) * (tokens // GRID_W)
        for which, gain_ref in enumerate((qg_ref, kg_ref)):
            gain = gain_ref[...]
            wide = jnp.broadcast_to(gain, (8, HEAD_DIM))
            other = jnp.where(low, pltpu.roll(wide, 96, 1)[0:1], pltpu.roll(wide, 32, 1)[0:1])
            for kind, scale in enumerate((gain, other)):
                for i in range(tokens // GRID_W):
                    at_row = row_ref[kind, pl.ds(start + i, 1), :]
                    table = jnp.where(lane < HEAD_DIM // 2, at_row, col_ref[kind])
                    table_ref[which, kind, i * GRID_W : (i + 1) * GRID_W, :] = table * scale

    ones = jnp.ones((HEAD_DIM, HEAD_DIM), BF16)
    raw = [q_ref[:, h * HEAD_DIM : (h + 1) * HEAD_DIM] for h in range(group)] + [k_ref[...]]
    raw = jnp.concatenate(raw, axis=0)
    floats = raw.astype(F32)
    square = floats * floats
    high = square.astype(BF16)
    low_part = (square - high.astype(F32)).astype(BF16)
    total = dot(high, ones) + dot(low_part, ones)
    scale = lax.rsqrt(total * (1.0 / HEAD_DIM) + EPSILON)
    other = dot(raw, swap_ref[...])
    value = v_ref[...]
    queries = [None] * group
    for h in range(group, -1, -1):
        rows = slice(h * tokens, (h + 1) * tokens)
        which = 1 if h == group else 0
        turned = floats[rows] * table_ref[which, 0] + other[rows] * table_ref[which, 1]
        turned = (turned * scale[rows]).astype(BF16)
        if h == group:
            for g in range(group):
                out_ref[g, :, HEAD_DIM : 2 * HEAD_DIM] = turned
                out_ref[g, :, 2 * HEAD_DIM : 3 * HEAD_DIM] = value
        else:
            queries[h] = turned
    queries = jnp.concatenate(queries, axis=1)
    queries = dot(sort_ref[...], queries).astype(BF16)
    for h in range(group):
        out_ref[h, :, 0:HEAD_DIM] = queries[:, h * HEAD_DIM : (h + 1) * HEAD_DIM]
    residual = dot(shift_ref[...], res_ref[...]).astype(BF16)
    span = res_ref.shape[1]
    cols = pl.ds(pl.multiple_of(pl.program_id(0) * span, span), span)
    for i, block_ref in enumerate(block_refs):
        block_ref[:, cols] = residual[32 * i : 32 * (i + 1)]


def attend_kernel(x_ref, out_ref, value_ref, even_ref, odd_ref):
    length = x_ref.shape[0]
    tokens = out_ref.shape[1]
    block = even_ref.shape[0]
    blocks = length // block
    value_ref[:, 0:HEAD_DIM] = x_ref[:, 2 * HEAD_DIM : 3 * HEAD_DIM]
    value_ref[:, HEAD_DIM:] = jnp.ones((length, HEAD_DIM), BF16)
    scale = float(HEAD_DIM ** (-0.5) * np.log2(np.e))

    def score(i, score_ref):
        rows = pl.ds(pl.multiple_of(i * block, block), block)
        score_ref[...] = dot(x_ref[rows, 0:HEAD_DIM], x_ref[:, HEAD_DIM : 2 * HEAD_DIM], ((1,), (1,)))

    def mix(i, score_ref):
        top = jnp.max(score_ref[...], axis=-1, keepdims=True)
        weights = jnp.exp2((score_ref[...] - top) * scale).astype(BF16)
        both = dot(weights, value_ref[...])
        made = (both[:, 0:HEAD_DIM] / both[:, HEAD_DIM:]).astype(BF16)
        part = tokens // 4
        for z in range(4):
            for g in range(4):
                at = z * tokens + g * part
                out_ref[4 * i + g, z * part : (z + 1) * part, :] = made[at : at + part]

    score(0, even_ref)

    def two(j, carry):
        i = 2 * j
        score(i + 1, odd_ref)
        mix(i, even_ref)
        score(jnp.minimum(i + 2, blocks - 1), even_ref)
        mix(i + 1, odd_ref)
        return carry

    lax.fori_loop(0, blocks // 2, two, 0)


def rms(floats, gain):
    return floats * lax.rsqrt(jnp.mean(floats * floats, axis=-1, keepdims=True) + EPSILON) * gain


def proj_kernel(place_ref, att_ref, w_ref, post_ref, pre_ref, *rest):
    block_refs = rest[:4]
    *_, out_ref, stream_ref, slot_ref, share_ref, x_ref, res_ref = rest
    tokens, width = x_ref.shape
    plane = lax.shift_right_logical(place_ref[0], 5)
    core = lax.bitwise_and(place_ref[0], 1)
    part = tokens // 4
    for shift, block_ref in enumerate(block_refs):
        home = lax.bitwise_and(plane - shift, 3)
        res_ref[pl.ds(pl.multiple_of(home * part, part), part), :] = block_ref[...]
    facts = res_ref[:, width:].astype(F32)
    weight = facts[:, 2:3] + facts[:, 3:4] + facts[:, 4:5]
    share = facts[:, 5:6] + facts[:, 6:7] + facts[:, 7:8]
    lane = lax.broadcasted_iota(jnp.int32, (tokens, HEAD_DIM), 1)
    share_ref[...] = jnp.where(lane == 0, weight * share, weight * (1.0 - share))
    turned = facts.T
    local_ids = [lax.bitwise_and(turned[i : i + 1].astype(jnp.int32), 31) for i in range(2)]
    which = lax.broadcasted_iota(jnp.int32, (32, tokens), 0)
    hits = [jnp.where(which == one, 1.0, 0.0) for one in local_ids]
    rank = dot((hits[0] + hits[1]).astype(BF16), earlier(tokens, 5))
    home = lax.shift_right_logical(lax.broadcasted_iota(jnp.int32, (1, tokens), 1), 5)
    slots = []
    for i in range(2):
        mine = jnp.sum(rank * hits[i], axis=0, keepdims=True).astype(jnp.int32)
        expert = local_ids[i]
        x_place = lax.shift_right_logical(expert, 3)
        y_place = lax.bitwise_and(lax.shift_right_logical(expert, 1), 3)
        side = lax.bitwise_xor(lax.bitwise_and(expert, 1), core)
        slots.append((y_place * 4 + x_place) * 32 + side * 16 + home * CAP + mine)
        slot_ref[i : i + 1, :] = slots[i]
    slot = lax.broadcasted_iota(jnp.int32, (4 * tokens, tokens), 0)
    picks = jnp.where((slot == slots[0]) | (slot == slots[1]), 1.0, 0.0).astype(BF16)
    for h in range(HEADS):
        x_ref[:, h * HEAD_DIM : (h + 1) * HEAD_DIM] = att_ref[h]
    mixed = dot(x_ref[...], w_ref[...]).astype(BF16).astype(F32)
    residual = res_ref[:, 0:width].astype(F32)
    stream = (residual + rms(mixed, post_ref[...])).astype(BF16)
    stream_ref[...] = stream
    normed = rms(stream.astype(F32), pre_ref[...]).astype(BF16)
    out_ref[...] = dot(picks, normed).astype(BF16).reshape(out_ref.shape)


def expert_kernel(y_ref, *rest):
    *weights, out_ref = rest
    peers, rows, width = y_ref.shape
    half = rows // 2
    for side in range(2):
        gate_ref, up_ref, down_ref = weights[3 * side : 3 * side + 3]
        span = slice(side * half, (side + 1) * half)
        x = y_ref[:, span, :].reshape(peers * half, width)
        gated = dot(x, gate_ref[...])
        lifted = dot(x, up_ref[...])
        hidden = (gated / (1.0 + jnp.exp(-gated)) * lifted).astype(BF16)
        made = dot(hidden, down_ref[...]).astype(BF16)
        out_ref[:, span, :] = made.reshape(peers, half, width)


def combine_kernel(z_ref, stream_ref, slot_ref, share_ref, out_ref):
    slots = z_ref.shape[0]
    tokens, width = stream_ref.shape
    slot = lax.broadcasted_iota(jnp.int32, (slots, tokens), 0)
    picks = [jnp.where(slot == slot_ref[i : i + 1, :], 1.0, 0.0).astype(BF16) for i in range(2)]
    picked = dot(jnp.concatenate(picks, axis=1), z_ref[...], ((0,), (0,)))
    ffn = share_ref[:, 0:1] * picked[0:tokens] + share_ref[:, 1:2] * picked[tokens:]
    out_ref[...] = (stream_ref[...].astype(F32) + ffn).astype(BF16)


def home_kernel(rows_ref, ids_ref, out_ref):
    tokens = out_ref.shape[0]
    row = lax.broadcasted_iota(jnp.int32, (tokens, tokens), 0)
    sort = jnp.where(row == group_positions(ids_ref), 1.0, 0.0).astype(BF16)
    out_ref[...] = dot(sort, rows_ref[...], ((0,), (0,))).astype(BF16)


def local(
    residual_in,
    query_proj,
    key_proj,
    value_proj,
    query_gain,
    key_gain,
    out_weight,
    post_gain,
    pre_gain,
    route_ids,
    group_weight,
    first_share,
    gate_weight,
    up_weight,
    down_weight,
):
    line = ("x", "z")
    sp_count = lax.axis_size(line)
    tokens, width = query_proj.shape[1:]
    length = tokens * sp_count
    chips = sp_count * lax.axis_size("y")
    experts = 2 * chips
    assert sp_count == HEADS and gate_weight.shape[0] == 1 and lax.axis_size("core") == 2
    place = lax.axis_index(("z", "x", "y", "core")).astype(jnp.int32).reshape(1)
    row_table = jnp.asarray(angle_tables(length // GRID_W))
    col_table = jnp.asarray(angle_tables(GRID_W))
    swap_table = jnp.asarray(partner_matrix(), BF16)
    swap = [(0, 1), (1, 0)]
    own = (gate_weight[0], up_weight[0], down_weight[0])

    vmem = pl.BlockSpec(memory_space=pltpu.VMEM)
    smem = pl.BlockSpec(memory_space=pltpu.SMEM)
    limit = lambda mib: pltpu.CompilerParams(vmem_limit_bytes=mib * 2**20)
    group = HEADS // KV_HEADS
    fixed = lambda *shape: pl.BlockSpec(shape, lambda n: (0,) * len(shape))
    ids = route_ids[0].T
    wide = width + HEAD_DIM
    assert tokens == 128 and width == HEADS * HEAD_DIM and experts == 128
    packed, *blocks = pl.pallas_call(
        pack_kernel,
        grid=(KV_HEADS,),
        out_shape=(
            jax.ShapeDtypeStruct((HEADS, tokens, 3 * HEAD_DIM), BF16),
            *[jax.ShapeDtypeStruct((tokens // 4, wide), BF16)] * 4,
        ),
        in_specs=[
            smem,
            pl.BlockSpec((tokens, group * HEAD_DIM), lambda n: (0, n)),
            pl.BlockSpec((tokens, HEAD_DIM), lambda n: (0, n)),
            pl.BlockSpec((tokens, HEAD_DIM), lambda n: (0, n)),
            pl.BlockSpec((tokens, width // KV_HEADS), lambda n: (0, n)),
            fixed(1, HEAD_DIM),
            fixed(1, HEAD_DIM),
            fixed(*row_table.shape),
            fixed(*col_table.shape),
            fixed(*swap_table.shape),
            fixed(2, tokens),
            fixed(1, tokens),
            fixed(1, tokens),
        ],
        out_specs=(
            pl.BlockSpec((group, tokens, 3 * HEAD_DIM), lambda n: (n, 0, 0)),
            *[fixed(tokens // 4, wide)] * 4,
        ),
        scratch_shapes=[
            pltpu.VMEM((2, 2, tokens, HEAD_DIM), F32),
            pltpu.VMEM((tokens, tokens), BF16),
            pltpu.VMEM((tokens, tokens), BF16),
        ],
        compiler_params=limit(58),
        name="pack",
    )(
        place,
        query_proj[0],
        key_proj[0],
        value_proj[0],
        residual_in[0],
        query_gain[None],
        key_gain[None],
        row_table,
        col_table,
        swap_table,
        ids,
        group_weight,
        first_share,
    )
    gathered = lax.all_to_all(packed, line, 0, 0, tiled=True)
    gathered, *held = lax.optimization_barrier((gathered, *own, *blocks[1:]))
    partner = tuple(lax.ppermute(one, "core", swap) for one in held[:3])
    for shift in range(1, 4):
        ring = [(i, (i + shift) % 4) for i in range(4)]
        blocks[shift] = lax.ppermute(held[2 + shift], "z", ring)
    block = 512
    attended = pl.pallas_call(
        attend_kernel,
        out_shape=jax.ShapeDtypeStruct((sp_count, tokens, HEAD_DIM), BF16),
        in_specs=[vmem],
        out_specs=vmem,
        scratch_shapes=[
            pltpu.VMEM((length, 2 * HEAD_DIM), BF16),
            pltpu.VMEM((block, length), F32),
            pltpu.VMEM((block, length), F32),
        ],
        compiler_params=limit(24),
        cost_estimate=pl.CostEstimate(
            flops=4 * length * length * HEAD_DIM * 4,
            bytes_accessed=length * HEAD_DIM * 8,
            transcendentals=length * length,
        ),
        name="attend",
    )(gathered.reshape(length, 3 * HEAD_DIM))
    attended, *blocks[1:] = lax.optimization_barrier((attended, *blocks[1:]))
    attended = lax.all_to_all(attended, line, 0, 0, tiled=True)
    hbm = pl.BlockSpec(memory_space=pltpu.HBM)
    chunk = (16, 4 * tokens // 16, width)
    sent, stream, slots, shares = pl.pallas_call(
        proj_kernel,
        out_shape=(
            jax.ShapeDtypeStruct(chunk, BF16),
            jax.ShapeDtypeStruct((tokens, width), BF16),
            jax.ShapeDtypeStruct((8, tokens), jnp.int32),
            jax.ShapeDtypeStruct((tokens, HEAD_DIM), F32),
        ),
        in_specs=[smem] + [vmem] * 8 + [hbm] * 3,
        out_specs=(vmem,) * 4,
        scratch_shapes=[pltpu.VMEM((tokens, width), BF16), pltpu.VMEM((tokens, wide), BF16)],
        compiler_params=limit(24),
        name="project",
    )(place, attended, out_weight, post_gain[None], pre_gain[None], *blocks, *partner)
    peers = ("y", "x")
    arrived = lax.all_to_all(sent, peers, 0, 0, tiled=True)
    answered = pl.pallas_call(
        expert_kernel,
        out_shape=jax.ShapeDtypeStruct(chunk, BF16),
        in_specs=[vmem] * 7,
        out_specs=vmem,
        compiler_params=limit(24),
        name="expert",
    )(arrived, *own, *partner)
    returned = lax.all_to_all(answered, peers, 0, 0, tiled=True)
    combined = pl.pallas_call(
        combine_kernel,
        out_shape=jax.ShapeDtypeStruct((tokens, width), BF16),
        in_specs=[vmem] * 4,
        out_specs=vmem,
        compiler_params=limit(16),
        name="combine",
    )(returned.reshape(4 * tokens, width), stream, slots, shares)
    finished = lax.all_to_all(combined.reshape(4, tokens // 4, width), "z", 0, 0, tiled=True)
    layer_out = pl.pallas_call(
        home_kernel,
        out_shape=jax.ShapeDtypeStruct((tokens, width), BF16),
        in_specs=[vmem] * 2,
        out_specs=vmem,
        compiler_params=limit(16),
        name="home",
    )(finished.reshape(tokens, width), ids)
    return layer_out[None]


def solution(mesh):
    assert mesh.devices.shape == (16, 8)
    grid = mesh.devices.reshape(4, 4, 4, 2)
    mesh = Mesh(grid, ("z", "x", "y", "core"))
    placed = (
        P(("y", "core"), ("z", "x"), None),
        P(("y", "core"), ("z", "x"), None),
        P(("y", "core"), ("z", "x"), None),
        P(("y", "core"), ("z", "x"), None),
        P(),
        P(),
        P(),
        P(),
        P(),
        P(("y", "core"), ("z", "x"), None),
        P(("y", "core"), ("z", "x")),
        P(("y", "core"), ("z", "x")),
        P(("z", "x", "y", "core"), None, None),
        P(("z", "x", "y", "core"), None, None),
        P(("z", "x", "y", "core"), None, None),
    )
    return jax.shard_map(
        local, mesh=mesh, in_specs=placed, out_specs=P(("y", "core"), ("z", "x"), None), check_vma=False
    )
```

```python
import functools

import jax
import jax.numpy as jnp
import numpy as np
from jax import lax
from jax.experimental import pallas as pl
from jax.experimental.pallas import tpu as pltpu
from jax.sharding import Mesh
from jax.sharding import PartitionSpec as P

HEADS = 16
KV_HEADS = 4
HEAD_DIM = 128
GRID_W = 64
CAP = 4
EPSILON = 1e-06
LATE_CORE = 0
STAGGER_NS = 8000
F32 = jnp.float32
BF16 = jnp.bfloat16


def dot(a, b, dims=((1,), (0,))):
    return lax.dot_general(a, b, (dims, ((), ())), preferred_element_type=F32)


def angle_tables(count):
    quarter = HEAD_DIM // 4
    inverse = np.float32(10000.0) ** (-np.arange(quarter, dtype=np.float32) / np.float32(quarter))
    angles = np.arange(count, dtype=np.float32)[:, None] * inverse.astype(np.float32)
    angles = np.tile(angles.astype(np.float64), (1, 4))
    return np.stack([np.cos(angles), np.sin(angles)]).astype(np.float32)


def partner_matrix():
    lane = np.arange(HEAD_DIM)
    low = (lane & 32) == 0
    matrix = np.zeros((HEAD_DIM, HEAD_DIM), np.float32)
    matrix[np.where(low, lane + 32, lane - 32), lane] = np.where(low, -1.0, 1.0)
    return matrix


def pack_kernel(
    place_ref, q_ref, k_ref, v_ref, qg_ref, kg_ref, row_ref, col_ref, swap_ref, out_ref, table_ref
):
    tokens = k_ref.shape[0]
    group = out_ref.shape[0]
    late = lax.bitwise_and(place_ref[0], 1) == LATE_CORE

    @pl.when((pl.program_id(0) == 0) & late)
    def _():
        pl.delay(STAGGER_NS)

    @pl.when(pl.program_id(0) == 0)
    def _():
        lane = lax.broadcasted_iota(jnp.int32, (GRID_W, HEAD_DIM), 1)
        line = lax.broadcasted_iota(jnp.int32, (1, HEAD_DIM), 1)
        low = lax.bitwise_and(line, 32) == 0
        start = lax.shift_right_logical(place_ref[0], 3) * (tokens // GRID_W)
        for which, gain_ref in enumerate((qg_ref, kg_ref)):
            gain = gain_ref[...]
            wide = jnp.broadcast_to(gain, (8, HEAD_DIM))
            other = jnp.where(low, pltpu.roll(wide, 96, 1)[0:1], pltpu.roll(wide, 32, 1)[0:1])
            for kind, scale in enumerate((gain, other)):
                for i in range(tokens // GRID_W):
                    at_row = row_ref[kind, pl.ds(start + i, 1), :]
                    table = jnp.where(lane < HEAD_DIM // 2, at_row, col_ref[kind])
                    table_ref[which, kind, i * GRID_W : (i + 1) * GRID_W, :] = table * scale

    ones = jnp.ones((HEAD_DIM, HEAD_DIM), BF16)
    raw = [q_ref[:, h * HEAD_DIM : (h + 1) * HEAD_DIM] for h in range(group)] + [k_ref[...]]
    raw = jnp.concatenate(raw, axis=0)
    floats = raw.astype(F32)
    square = floats * floats
    high = square.astype(BF16)
    low_part = (square - high.astype(F32)).astype(BF16)
    total = dot(high, ones) + dot(low_part, ones)
    scale = lax.rsqrt(total * (1.0 / HEAD_DIM) + EPSILON)
    other = dot(raw, swap_ref[...])
    value = v_ref[...]
    for h in range(group, -1, -1):
        rows = slice(h * tokens, (h + 1) * tokens)
        which = 1 if h == group else 0
        turned = floats[rows] * table_ref[which, 0] + other[rows] * table_ref[which, 1]
        turned = (turned * scale[rows]).astype(BF16)
        if h == group:
            for g in range(group):
                out_ref[g, :, HEAD_DIM : 2 * HEAD_DIM] = turned
                out_ref[g, :, 2 * HEAD_DIM : 3 * HEAD_DIM] = value
        else:
            out_ref[h, :, 0:HEAD_DIM] = turned


def attend_kernel(x_ref, out_ref, value_ref, even_ref, odd_ref):
    length = x_ref.shape[0]
    block = even_ref.shape[0]
    blocks = length // block
    value_ref[:, 0:HEAD_DIM] = x_ref[:, 2 * HEAD_DIM : 3 * HEAD_DIM]
    value_ref[:, HEAD_DIM:] = jnp.ones((length, HEAD_DIM), BF16)
    scale = float(HEAD_DIM ** (-0.5) * np.log2(np.e))

    def score(i, score_ref):
        rows = pl.ds(pl.multiple_of(i * block, block), block)
        score_ref[...] = dot(x_ref[rows, 0:HEAD_DIM], x_ref[:, HEAD_DIM : 2 * HEAD_DIM], ((1,), (1,)))

    def mix(i, score_ref):
        rows = pl.ds(pl.multiple_of(i * block, block), block)
        top = jnp.max(score_ref[...], axis=-1, keepdims=True)
        weights = jnp.exp2((score_ref[...] - top) * scale).astype(BF16)
        both = dot(weights, value_ref[...])
        out_ref[rows, :] = (both[:, 0:HEAD_DIM] / both[:, HEAD_DIM:]).astype(BF16)

    score(0, even_ref)

    def two(j, carry):
        i = 2 * j
        score(i + 1, odd_ref)
        mix(i, even_ref)
        score(jnp.minimum(i + 2, blocks - 1), even_ref)
        mix(i + 1, odd_ref)
        return carry

    lax.fori_loop(0, blocks // 2, two, 0)


def rms(floats, gain):
    return floats * lax.rsqrt(jnp.mean(floats * floats, axis=-1, keepdims=True) + EPSILON) * gain


def proj_kernel(place_ref, att_ref, w_ref, res_ref, post_ref, pre_ref, ids_ref, *rest):
    *_, out_ref, stream_ref, slot_ref, x_ref = rest
    tokens, width = x_ref.shape
    for h in range(HEADS):
        x_ref[:, h * HEAD_DIM : (h + 1) * HEAD_DIM] = att_ref[h]
    experts = 2 * out_ref.shape[0]
    which = lax.broadcasted_iota(jnp.int32, (experts, tokens), 0)
    first = ids_ref[0:1, :]
    second = ids_ref[1:2, :]
    hit_first = jnp.where(which == first, 1.0, 0.0)
    hit_second = jnp.where(which == second, 1.0, 0.0)
    row = lax.broadcasted_iota(jnp.int32, (tokens, tokens), 0)
    col = lax.broadcasted_iota(jnp.int32, (tokens, tokens), 1)
    before = jnp.where(row < col, 1.0, 0.0).astype(BF16)
    rank = dot((hit_first + hit_second).astype(BF16), before)
    rank_first = jnp.sum(rank * hit_first, axis=0, keepdims=True).astype(jnp.int32)
    rank_second = jnp.sum(rank * hit_second, axis=0, keepdims=True).astype(jnp.int32)
    core = lax.bitwise_and(place_ref[0], 1)

    def slot_of(expert, rank):
        side = lax.bitwise_xor(lax.bitwise_and(expert, 1), core)
        return lax.shift_right_logical(expert, 1) * (2 * CAP) + rank * 2 + side

    slot_first = slot_of(first, rank_first)
    slot_second = slot_of(second, rank_second)
    slot_ref[0:1, :] = slot_first
    slot_ref[1:2, :] = slot_second
    slot = lax.broadcasted_iota(jnp.int32, (experts * CAP, tokens), 0)
    here = (slot == slot_first) | (slot == slot_second)
    picks = jnp.where(here, 1.0, 0.0).astype(BF16)
    mixed = dot(x_ref[...], w_ref[...]).astype(BF16).astype(F32)
    stream = (res_ref[...].astype(F32) + rms(mixed, post_ref[...])).astype(BF16)
    stream_ref[...] = stream
    normed = rms(stream.astype(F32), pre_ref[...]).astype(BF16)
    out_ref[...] = dot(picks, normed).astype(BF16).reshape(out_ref.shape)


def expert_kernel(y_ref, *rest):
    weights, late, (out_ref, wide_ref, x_ref, *held, sems) = list(rest[:4]), rest[4:6], rest[6:]
    copies = [pltpu.make_async_copy(late[i], held[i], sems.at[i]) for i in range(2)]
    for copy in copies:
        copy.start()
    weights += held
    slots, width = y_ref.shape
    sides = [pl.ds(side, slots // 2, stride=2) for side in range(2)]
    blocks = [slice(c * 128, (c + 1) * 128) for c in range(width // 128)]
    for c, cols in enumerate(blocks):
        wide_ref[c] = y_ref[:, cols].astype(F32)
        for side in range(2):
            x_ref[side, :, cols] = wide_ref[c, sides[side], :].astype(BF16)
    for side in range(2):
        gate_ref, up_ref, down_ref = weights[3 * side : 3 * side + 3]
        gated = dot(x_ref[side], gate_ref[...])
        if side == 1:
            copies[0].wait()
        lifted = dot(x_ref[side], up_ref[...])
        hidden = (gated / (1.0 + jnp.exp(-gated)) * lifted).astype(BF16)
        if side == 1:
            copies[1].wait()
        made = dot(hidden, down_ref[...])
        for c, cols in enumerate(blocks):
            wide_ref[c, sides[side], :] = made[:, cols]
    for c, cols in enumerate(blocks):
        out_ref[:, cols] = wide_ref[c].astype(BF16)


def combine_kernel(z_ref, stream_ref, slot_ref, weight_ref, share_ref, out_ref):
    slots = z_ref.shape[0]
    tokens, width = stream_ref.shape
    slot = lax.broadcasted_iota(jnp.int32, (slots, tokens), 0)
    picks = [jnp.where(slot == slot_ref[i : i + 1, :], 1.0, 0.0).astype(BF16) for i in range(2)]
    picked = dot(jnp.concatenate(picks, axis=1), z_ref[...], ((0,), (0,)))
    column = lambda row: jnp.broadcast_to(row, (tokens, tokens)).T[:, 0:1]
    weight = weight_ref[...]
    share = share_ref[...]
    weight_first = column(weight * share)
    weight_second = column(weight * (1.0 - share))
    ffn = weight_first * picked[0:tokens] + weight_second * picked[tokens:]
    out_ref[...] = (stream_ref[...].astype(F32) + ffn).astype(BF16)


def local(
    residual_in,
    query_proj,
    key_proj,
    value_proj,
    query_gain,
    key_gain,
    out_weight,
    post_gain,
    pre_gain,
    route_ids,
    group_weight,
    first_share,
    gate_weight,
    up_weight,
    down_weight,
):
    line = ("x", "z")
    sp_count = lax.axis_size(line)
    tokens, width = query_proj.shape[1:]
    length = tokens * sp_count
    chips = sp_count * lax.axis_size("y")
    experts = 2 * chips
    assert sp_count == HEADS and gate_weight.shape[0] == 1 and lax.axis_size("core") == 2
    place = lax.axis_index(("z", "x", "y", "core")).astype(jnp.int32).reshape(1)
    row_table = jnp.asarray(angle_tables(length // GRID_W))
    col_table = jnp.asarray(angle_tables(GRID_W))
    swap_table = jnp.asarray(partner_matrix(), BF16)
    swap = [(0, 1), (1, 0)]
    own = (gate_weight[0], up_weight[0], down_weight[0])
    partner = tuple(lax.ppermute(one, "core", swap) for one in own)

    vmem = pl.BlockSpec(memory_space=pltpu.VMEM)
    smem = pl.BlockSpec(memory_space=pltpu.SMEM)
    limit = lambda mib: pltpu.CompilerParams(vmem_limit_bytes=mib * 2**20)
    group = HEADS // KV_HEADS
    fixed = lambda *shape: pl.BlockSpec(shape, lambda n: (0,) * len(shape))
    packed = pl.pallas_call(
        pack_kernel,
        grid=(KV_HEADS,),
        out_shape=jax.ShapeDtypeStruct((HEADS, tokens, 3 * HEAD_DIM), BF16),
        in_specs=[
            smem,
            pl.BlockSpec((tokens, group * HEAD_DIM), lambda n: (0, n)),
            pl.BlockSpec((tokens, HEAD_DIM), lambda n: (0, n)),
            pl.BlockSpec((tokens, HEAD_DIM), lambda n: (0, n)),
            fixed(1, HEAD_DIM),
            fixed(1, HEAD_DIM),
            fixed(*row_table.shape),
            fixed(*col_table.shape),
            fixed(*swap_table.shape),
        ],
        out_specs=pl.BlockSpec((group, tokens, 3 * HEAD_DIM), lambda n: (n, 0, 0)),
        scratch_shapes=[pltpu.VMEM((2, 2, tokens, HEAD_DIM), F32)],
        compiler_params=limit(63),
        name="pack",
    )(
        place,
        query_proj[0],
        key_proj[0],
        value_proj[0],
        query_gain[None],
        key_gain[None],
        row_table,
        col_table,
        swap_table,
    )
    gathered = lax.all_to_all(packed, line, 0, 0, tiled=True)
    block = 512
    attended = pl.pallas_call(
        attend_kernel,
        out_shape=jax.ShapeDtypeStruct((length, HEAD_DIM), BF16),
        in_specs=[vmem],
        out_specs=vmem,
        scratch_shapes=[
            pltpu.VMEM((length, 2 * HEAD_DIM), BF16),
            pltpu.VMEM((block, length), F32),
            pltpu.VMEM((block, length), F32),
        ],
        compiler_params=limit(24),
        cost_estimate=pl.CostEstimate(
            flops=length * length * HEAD_DIM,
            bytes_accessed=length * HEAD_DIM * 8,
            transcendentals=length * length,
        ),
        name="attend",
    )(gathered.reshape(length, 3 * HEAD_DIM))
    attended = lax.all_to_all(attended.reshape(sp_count, tokens, HEAD_DIM), line, 0, 0, tiled=True)
    hbm = pl.BlockSpec(memory_space=pltpu.HBM)
    sent, stream, slots = pl.pallas_call(
        proj_kernel,
        out_shape=(
            jax.ShapeDtypeStruct((chips, 2 * CAP, width), BF16),
            jax.ShapeDtypeStruct((tokens, width), BF16),
            jax.ShapeDtypeStruct((8, tokens), jnp.int32),
        ),
        in_specs=[smem] + [vmem] * 6 + [hbm] * 3,
        out_specs=(vmem,) * 3,
        scratch_shapes=[
            pltpu.VMEM((tokens, width), BF16),
        ],
        compiler_params=limit(24),
        name="project",
    )(
        place,
        attended,
        out_weight,
        residual_in[0],
        post_gain[None],
        pre_gain[None],
        route_ids[0].T,
        *partner,
    )
    peers = ("z", "x", "y")
    arrived = lax.all_to_all(sent, peers, 0, 0, tiled=True)
    rows = experts * CAP
    answered = pl.pallas_call(
        expert_kernel,
        out_shape=jax.ShapeDtypeStruct((rows, width), BF16),
        in_specs=[vmem] * 5 + [hbm] * 2,
        out_specs=vmem,
        scratch_shapes=[
            pltpu.VMEM((width // 128, rows, 128), F32),
            pltpu.VMEM((2, rows // 2, width), BF16),
            *[pltpu.VMEM(one.shape, BF16) for one in partner[1:]],
            pltpu.SemaphoreType.DMA((2,)),
        ],
        compiler_params=limit(24),
        name="expert",
    )(arrived.reshape(rows, width), *own, *partner)
    returned = lax.all_to_all(answered.reshape(chips, 2 * CAP, width), peers, 0, 0, tiled=True)
    combined = pl.pallas_call(
        combine_kernel,
        out_shape=jax.ShapeDtypeStruct((tokens, width), BF16),
        in_specs=[vmem] * 5,
        out_specs=vmem,
        compiler_params=limit(16),
        name="combine",
    )(returned.reshape(rows, width), stream, slots, group_weight, first_share)
    return combined[None]


def solution(mesh):
    assert mesh.devices.shape == (16, 8)
    grid = mesh.devices.reshape(4, 4, 4, 2)
    mesh = Mesh(grid, ("z", "x", "y", "core"))
    placed = (
        P(("y", "core"), ("z", "x"), None),
        P(("y", "core"), ("z", "x"), None),
        P(("y", "core"), ("z", "x"), None),
        P(("y", "core"), ("z", "x"), None),
        P(),
        P(),
        P(),
        P(),
        P(),
        P(("y", "core"), ("z", "x"), None),
        P(("y", "core"), ("z", "x")),
        P(("y", "core"), ("z", "x")),
        P(("z", "x", "y", "core"), None, None),
        P(("z", "x", "y", "core"), None, None),
        P(("z", "x", "y", "core"), None, None),
    )
    return jax.shard_map(
        local, mesh=mesh, in_specs=placed, out_specs=P(("y", "core"), ("z", "x"), None), check_vma=False
    )
```

```python
import functools

import jax
import jax.numpy as jnp
import numpy as np
from jax import lax
from jax.experimental import pallas as pl
from jax.experimental.pallas import tpu as pltpu
from jax.sharding import Mesh
from jax.sharding import PartitionSpec as P

HEADS = 16
KV_HEADS = 4
HEAD_DIM = 128
GRID_W = 64
CAP = 4
EPSILON = 1e-06
LATE_CORE = 0
PACK_STEPS = 2
STAGGER_NS = 8200
F32 = jnp.float32
BF16 = jnp.bfloat16


def dot(a, b, dims=((1,), (0,))):
    return lax.dot_general(a, b, (dims, ((), ())), preferred_element_type=F32)


def angle_tables(count):
    quarter = HEAD_DIM // 4
    inverse = np.float32(10000.0) ** (-np.arange(quarter, dtype=np.float32) / np.float32(quarter))
    angles = np.arange(count, dtype=np.float32)[:, None] * inverse.astype(np.float32)
    angles = np.tile(angles.astype(np.float64), (1, 4))
    return np.stack([np.cos(angles), np.sin(angles)]).astype(np.float32)


def partner_matrix():
    lane = np.arange(HEAD_DIM)
    low = (lane & 32) == 0
    matrix = np.zeros((HEAD_DIM, HEAD_DIM), np.float32)
    matrix[np.where(low, lane + 32, lane - 32), lane] = np.where(low, -1.0, 1.0)
    return matrix


def pack_kernel(
    place_ref, q_ref, k_ref, v_ref, qg_ref, kg_ref, row_ref, col_ref, swap_ref, out_ref, table_ref
):
    tokens = k_ref.shape[0]
    late = lax.bitwise_and(place_ref[0], 1) == LATE_CORE

    @pl.when((pl.program_id(0) == 0) & late)
    def _():
        pl.delay(STAGGER_NS)

    @pl.when(pl.program_id(0) == 0)
    def _():
        lane = lax.broadcasted_iota(jnp.int32, (GRID_W, HEAD_DIM), 1)
        line = lax.broadcasted_iota(jnp.int32, (1, HEAD_DIM), 1)
        low = lax.bitwise_and(line, 32) == 0
        start = lax.shift_right_logical(place_ref[0], 3) * (tokens // GRID_W)
        for which, gain_ref in enumerate((qg_ref, kg_ref)):
            gain = gain_ref[...]
            wide = jnp.broadcast_to(gain, (8, HEAD_DIM))
            other = jnp.where(low, pltpu.roll(wide, 96, 1)[0:1], pltpu.roll(wide, 32, 1)[0:1])
            for kind, scale in enumerate((gain, other)):
                for i in range(tokens // GRID_W):
                    at_row = row_ref[kind, pl.ds(start + i, 1), :]
                    table = jnp.where(lane < HEAD_DIM // 2, at_row, col_ref[kind])
                    table_ref[which, kind, i * GRID_W : (i + 1) * GRID_W, :] = table * scale

    ones = jnp.ones((HEAD_DIM, HEAD_DIM), BF16)
    keys = k_ref.shape[1] // HEAD_DIM
    group = HEADS // KV_HEADS
    head = lambda ref, h: ref[:, h * HEAD_DIM : (h + 1) * HEAD_DIM]
    raw = [head(q_ref, h) for h in range(keys * group)] + [head(k_ref, kv) for kv in range(keys)]
    raw = jnp.concatenate(raw, axis=0)
    floats = raw.astype(F32)
    square = floats * floats
    high = square.astype(BF16)
    low_part = (square - high.astype(F32)).astype(BF16)
    total = dot(high, ones) + dot(low_part, ones)
    scale = lax.rsqrt(total * (1.0 / HEAD_DIM) + EPSILON)
    other = dot(raw, swap_ref[...])
    for h in range(keys * (group + 1)):
        rows = slice(h * tokens, (h + 1) * tokens)
        which = 1 if h >= keys * group else 0
        turned = floats[rows] * table_ref[which, 0] + other[rows] * table_ref[which, 1]
        turned = (turned * scale[rows]).astype(BF16)
        if which == 0:
            out_ref[h, :, 0:HEAD_DIM] = turned
            continue
        kv = h - keys * group
        for g in range(kv * group, (kv + 1) * group):
            out_ref[g, :, HEAD_DIM : 2 * HEAD_DIM] = turned
            out_ref[g, :, 2 * HEAD_DIM : 3 * HEAD_DIM] = head(v_ref, kv)


def attend_kernel(x_ref, out_ref, value_ref, even_ref, odd_ref):
    length = x_ref.shape[0]
    block = even_ref.shape[0]
    blocks = length // block
    value_ref[:, 0:HEAD_DIM] = x_ref[:, 2 * HEAD_DIM : 3 * HEAD_DIM]
    value_ref[:, HEAD_DIM:] = jnp.ones((length, HEAD_DIM), BF16)
    scale = float(HEAD_DIM ** (-0.5) * np.log2(np.e))

    def score(i, score_ref):
        rows = pl.ds(pl.multiple_of(i * block, block), block)
        score_ref[...] = dot(x_ref[rows, 0:HEAD_DIM], x_ref[:, HEAD_DIM : 2 * HEAD_DIM], ((1,), (1,)))

    def mix(i, score_ref):
        rows = pl.ds(pl.multiple_of(i * block, block), block)
        top = jnp.max(score_ref[...], axis=-1, keepdims=True)
        weights = jnp.exp2((score_ref[...] - top) * scale).astype(BF16)
        both = dot(weights, value_ref[...])
        out_ref[rows, :] = (both[:, 0:HEAD_DIM] / both[:, HEAD_DIM:]).astype(BF16)

    score(0, even_ref)

    def two(j, carry):
        i = 2 * j
        score(i + 1, odd_ref)
        mix(i, even_ref)
        score(jnp.minimum(i + 2, blocks - 1), even_ref)
        mix(i + 1, odd_ref)
        return carry

    lax.fori_loop(0, blocks // 2, two, 0)


def rms(floats, gain):
    return floats * lax.rsqrt(jnp.mean(floats * floats, axis=-1, keepdims=True) + EPSILON) * gain


def proj_kernel(place_ref, att_ref, w_ref, res_ref, post_ref, pre_ref, ids_ref, *rest):
    *_, out_ref, stream_ref, slot_ref, x_ref = rest
    tokens, width = x_ref.shape
    for h in range(HEADS):
        x_ref[:, h * HEAD_DIM : (h + 1) * HEAD_DIM] = att_ref[h]
    experts = 2 * out_ref.shape[0]
    which = lax.broadcasted_iota(jnp.int32, (experts, tokens), 0)
    first = ids_ref[0:1, :]
    second = ids_ref[1:2, :]
    hit_first = jnp.where(which == first, 1.0, 0.0)
    hit_second = jnp.where(which == second, 1.0, 0.0)
    row = lax.broadcasted_iota(jnp.int32, (tokens, tokens), 0)
    col = lax.broadcasted_iota(jnp.int32, (tokens, tokens), 1)
    before = jnp.where(row < col, 1.0, 0.0).astype(BF16)
    rank = dot((hit_first + hit_second).astype(BF16), before)
    rank_first = jnp.sum(rank * hit_first, axis=0, keepdims=True).astype(jnp.int32)
    rank_second = jnp.sum(rank * hit_second, axis=0, keepdims=True).astype(jnp.int32)
    core = lax.bitwise_and(place_ref[0], 1)

    def slot_of(expert, rank):
        side = lax.bitwise_xor(lax.bitwise_and(expert, 1), core)
        return lax.shift_right_logical(expert, 1) * (2 * CAP) + rank * 2 + side

    slot_first = slot_of(first, rank_first)
    slot_second = slot_of(second, rank_second)
    slot_ref[0:1, :] = slot_first
    slot_ref[1:2, :] = slot_second
    slot = lax.broadcasted_iota(jnp.int32, (experts * CAP, tokens), 0)
    here = (slot == slot_first) | (slot == slot_second)
    picks = jnp.where(here, 1.0, 0.0).astype(BF16)
    mixed = dot(x_ref[...], w_ref[...]).astype(BF16).astype(F32)
    stream = (res_ref[...].astype(F32) + rms(mixed, post_ref[...])).astype(BF16)
    stream_ref[...] = stream
    normed = rms(stream.astype(F32), pre_ref[...]).astype(BF16)
    out_ref[...] = dot(picks, normed).astype(BF16).reshape(out_ref.shape)


def expert_kernel(y_ref, *rest):
    weights, late, (out_ref, wide_ref, x_ref, *held, sems) = list(rest[:3]), rest[3:6], rest[6:]
    copies = [pltpu.make_async_copy(late[i], held[i], sems.at[i]) for i in range(3)]
    for copy in copies:
        copy.start()
    weights += held
    slots, width = y_ref.shape
    sides = [pl.ds(side, slots // 2, stride=2) for side in range(2)]
    blocks = [slice(c * 128, (c + 1) * 128) for c in range(width // 128)]
    for c, cols in enumerate(blocks):
        wide_ref[c] = y_ref[:, cols].astype(F32)
        for side in range(2):
            x_ref[side, :, cols] = wide_ref[c, sides[side], :].astype(BF16)
    for side in range(2):
        gate_ref, up_ref, down_ref = weights[3 * side : 3 * side + 3]
        if side == 1:
            copies[0].wait()
        gated = dot(x_ref[side], gate_ref[...])
        if side == 1:
            copies[1].wait()
        lifted = dot(x_ref[side], up_ref[...])
        hidden = (gated / (1.0 + jnp.exp(-gated)) * lifted).astype(BF16)
        if side == 1:
            copies[2].wait()
        made = dot(hidden, down_ref[...])
        for c, cols in enumerate(blocks):
            wide_ref[c, sides[side], :] = made[:, cols]
    for c, cols in enumerate(blocks):
        out_ref[:, cols] = wide_ref[c].astype(BF16)


def combine_kernel(z_ref, stream_ref, slot_ref, weight_ref, share_ref, out_ref):
    slots = z_ref.shape[0]
    tokens, width = stream_ref.shape
    slot = lax.broadcasted_iota(jnp.int32, (slots, tokens), 0)
    picks = [jnp.where(slot == slot_ref[i : i + 1, :], 1.0, 0.0).astype(BF16) for i in range(2)]
    picked = dot(jnp.concatenate(picks, axis=1), z_ref[...], ((0,), (0,)))
    column = lambda row: jnp.broadcast_to(row, (tokens, tokens)).T[:, 0:1]
    weight = weight_ref[...]
    share = share_ref[...]
    weight_first = column(weight * share)
    weight_second = column(weight * (1.0 - share))
    ffn = weight_first * picked[0:tokens] + weight_second * picked[tokens:]
    out_ref[...] = (stream_ref[...].astype(F32) + ffn).astype(BF16)


def local(
    residual_in,
    query_proj,
    key_proj,
    value_proj,
    query_gain,
    key_gain,
    out_weight,
    post_gain,
    pre_gain,
    route_ids,
    group_weight,
    first_share,
    gate_weight,
    up_weight,
    down_weight,
):
    line = ("x", "z")
    sp_count = lax.axis_size(line)
    tokens, width = query_proj.shape[1:]
    length = tokens * sp_count
    chips = sp_count * lax.axis_size("y")
    experts = 2 * chips
    assert sp_count == HEADS and gate_weight.shape[0] == 1 and lax.axis_size("core") == 2
    place = lax.axis_index(("z", "x", "y", "core")).astype(jnp.int32).reshape(1)
    row_table = jnp.asarray(angle_tables(length // GRID_W))
    col_table = jnp.asarray(angle_tables(GRID_W))
    swap_table = jnp.asarray(partner_matrix(), BF16)
    swap = [(0, 1), (1, 0)]
    own = (gate_weight[0], up_weight[0], down_weight[0])
    partner = tuple(lax.ppermute(one, "core", swap) for one in own)

    vmem = pl.BlockSpec(memory_space=pltpu.VMEM)
    smem = pl.BlockSpec(memory_space=pltpu.SMEM)
    limit = lambda mib: pltpu.CompilerParams(vmem_limit_bytes=mib * 2**20)
    kv_width = key_proj.shape[2]
    fixed = lambda *shape: pl.BlockSpec(shape, lambda n: (0,) * len(shape))
    packed = pl.pallas_call(
        pack_kernel,
        grid=(PACK_STEPS,),
        out_shape=jax.ShapeDtypeStruct((HEADS, tokens, 3 * HEAD_DIM), BF16),
        in_specs=[
            smem,
            pl.BlockSpec((tokens, width // PACK_STEPS), lambda n: (0, n)),
            pl.BlockSpec((tokens, kv_width // PACK_STEPS), lambda n: (0, n)),
            pl.BlockSpec((tokens, kv_width // PACK_STEPS), lambda n: (0, n)),
            fixed(1, HEAD_DIM),
            fixed(1, HEAD_DIM),
            fixed(*row_table.shape),
            fixed(*col_table.shape),
            fixed(*swap_table.shape),
        ],
        out_specs=pl.BlockSpec((HEADS // PACK_STEPS, tokens, 3 * HEAD_DIM), lambda n: (n, 0, 0)),
        scratch_shapes=[pltpu.VMEM((2, 2, tokens, HEAD_DIM), F32)],
        compiler_params=limit(63),
        name="pack",
    )(
        place,
        query_proj[0],
        key_proj[0],
        value_proj[0],
        query_gain[None],
        key_gain[None],
        row_table,
        col_table,
        swap_table,
    )
    gathered = lax.all_to_all(packed, line, 0, 0, tiled=True)
    block = 512
    attended = pl.pallas_call(
        attend_kernel,
        out_shape=jax.ShapeDtypeStruct((length, HEAD_DIM), BF16),
        in_specs=[vmem],
        out_specs=vmem,
        scratch_shapes=[
            pltpu.VMEM((length, 2 * HEAD_DIM), BF16),
            pltpu.VMEM((block, length), F32),
            pltpu.VMEM((block, length), F32),
        ],
        compiler_params=limit(24),
        cost_estimate=pl.CostEstimate(
            flops=length * length * HEAD_DIM,
            bytes_accessed=length * HEAD_DIM * 8,
            transcendentals=length * length,
        ),
        name="attend",
    )(gathered.reshape(length, 3 * HEAD_DIM))
    attended = lax.all_to_all(attended.reshape(sp_count, tokens, HEAD_DIM), line, 0, 0, tiled=True)
    hbm = pl.BlockSpec(memory_space=pltpu.HBM)
    sent, stream, slots = pl.pallas_call(
        proj_kernel,
        out_shape=(
            jax.ShapeDtypeStruct((chips, 2 * CAP, width), BF16),
            jax.ShapeDtypeStruct((tokens, width), BF16),
            jax.ShapeDtypeStruct((8, tokens), jnp.int32),
        ),
        in_specs=[smem] + [vmem] * 6 + [hbm] * 3,
        out_specs=(vmem,) * 3,
        scratch_shapes=[
            pltpu.VMEM((tokens, width), BF16),
        ],
        compiler_params=limit(24),
        name="project",
    )(
        place,
        attended,
        out_weight,
        residual_in[0],
        post_gain[None],
        pre_gain[None],
        route_ids[0].T,
        *partner,
    )
    peers = ("z", "x", "y")
    arrived = lax.all_to_all(sent, peers, 0, 0, tiled=True)
    rows = experts * CAP
    answered = pl.pallas_call(
        expert_kernel,
        out_shape=jax.ShapeDtypeStruct((rows, width), BF16),
        in_specs=[vmem] * 4 + [hbm] * 3,
        out_specs=vmem,
        scratch_shapes=[
            pltpu.VMEM((width // 128, rows, 128), F32),
            pltpu.VMEM((2, rows // 2, width), BF16),
            *[pltpu.VMEM(one.shape, BF16) for one in partner],
            pltpu.SemaphoreType.DMA((3,)),
        ],
        compiler_params=limit(24),
        name="expert",
    )(arrived.reshape(rows, width), *own, *partner)
    returned = lax.all_to_all(answered.reshape(chips, 2 * CAP, width), peers, 0, 0, tiled=True)
    combined = pl.pallas_call(
        combine_kernel,
        out_shape=jax.ShapeDtypeStruct((tokens, width), BF16),
        in_specs=[vmem] * 5,
        out_specs=vmem,
        compiler_params=limit(16),
        name="combine",
    )(returned.reshape(rows, width), stream, slots, group_weight, first_share)
    return combined[None]


def solution(mesh):
    assert mesh.devices.shape == (16, 8)
    grid = mesh.devices.reshape(4, 4, 4, 2)
    mesh = Mesh(grid, ("z", "x", "y", "core"))
    placed = (
        P(("y", "core"), ("z", "x"), None),
        P(("y", "core"), ("z", "x"), None),
        P(("y", "core"), ("z", "x"), None),
        P(("y", "core"), ("z", "x"), None),
        P(),
        P(),
        P(),
        P(),
        P(),
        P(("y", "core"), ("z", "x"), None),
        P(("y", "core"), ("z", "x")),
        P(("y", "core"), ("z", "x")),
        P(("z", "x", "y", "core"), None, None),
        P(("z", "x", "y", "core"), None, None),
        P(("z", "x", "y", "core"), None, None),
    )
    return jax.shard_map(
        local, mesh=mesh, in_specs=placed, out_specs=P(("y", "core"), ("z", "x"), None), check_vma=False
    )
```

```python
import functools

import jax
import jax.numpy as jnp
import numpy as np
from jax import lax
from jax.experimental import pallas as pl
from jax.experimental.pallas import tpu as pltpu
from jax.sharding import Mesh
from jax.sharding import PartitionSpec as P

HEADS = 16
KV_HEADS = 4
HEAD_DIM = 128
GRID_W = 64
CAP = 4
EPSILON = 1e-06
LATE_CORE = 0
PACK_STEPS = 2
STAGGER_NS = 8200
F32 = jnp.float32
BF16 = jnp.bfloat16


def dot(a, b, dims=((1,), (0,))):
    return lax.dot_general(a, b, (dims, ((), ())), preferred_element_type=F32)


def angle_tables(count):
    quarter = HEAD_DIM // 4
    inverse = np.float32(10000.0) ** (-np.arange(quarter, dtype=np.float32) / np.float32(quarter))
    angles = np.arange(count, dtype=np.float32)[:, None] * inverse.astype(np.float32)
    angles = np.tile(angles.astype(np.float64), (1, 4))
    return np.stack([np.cos(angles), np.sin(angles)]).astype(np.float32)


def partner_matrix():
    lane = np.arange(HEAD_DIM)
    low = (lane & 32) == 0
    matrix = np.zeros((HEAD_DIM, HEAD_DIM), np.float32)
    matrix[np.where(low, lane + 32, lane - 32), lane] = np.where(low, -1.0, 1.0)
    return matrix


def pack_kernel(
    place_ref, q_ref, k_ref, v_ref, qg_ref, kg_ref, row_ref, col_ref, swap_ref, out_ref, table_ref
):
    tokens = k_ref.shape[0]
    late = lax.bitwise_and(place_ref[0], 1) == LATE_CORE

    @pl.when((pl.program_id(0) == 0) & late)
    def _():
        pl.delay(STAGGER_NS)

    @pl.when(pl.program_id(0) == 0)
    def _():
        lane = lax.broadcasted_iota(jnp.int32, (GRID_W, HEAD_DIM), 1)
        line = lax.broadcasted_iota(jnp.int32, (1, HEAD_DIM), 1)
        low = lax.bitwise_and(line, 32) == 0
        start = lax.shift_right_logical(place_ref[0], 3) * (tokens // GRID_W)
        for which, gain_ref in enumerate((qg_ref, kg_ref)):
            gain = gain_ref[...]
            wide = jnp.broadcast_to(gain, (8, HEAD_DIM))
            other = jnp.where(low, pltpu.roll(wide, 96, 1)[0:1], pltpu.roll(wide, 32, 1)[0:1])
            for kind, scale in enumerate((gain, other)):
                for i in range(tokens // GRID_W):
                    at_row = row_ref[kind, pl.ds(start + i, 1), :]
                    table = jnp.where(lane < HEAD_DIM // 2, at_row, col_ref[kind])
                    table_ref[which, kind, i * GRID_W : (i + 1) * GRID_W, :] = table * scale

    ones = jnp.ones((HEAD_DIM, HEAD_DIM), BF16)
    keys = k_ref.shape[1] // HEAD_DIM
    group = HEADS // KV_HEADS
    head = lambda ref, h: ref[:, h * HEAD_DIM : (h + 1) * HEAD_DIM]
    raw = [head(q_ref, h) for h in range(keys * group)] + [head(k_ref, kv) for kv in range(keys)]
    raw = jnp.concatenate(raw, axis=0)
    floats = raw.astype(F32)
    square = floats * floats
    high = square.astype(BF16)
    low_part = (square - high.astype(F32)).astype(BF16)
    total = dot(high, ones) + dot(low_part, ones)
    scale = lax.rsqrt(total * (1.0 / HEAD_DIM) + EPSILON)
    other = dot(raw, swap_ref[...])
    for h in range(keys * (group + 1)):
        rows = slice(h * tokens, (h + 1) * tokens)
        which = 1 if h >= keys * group else 0
        turned = floats[rows] * table_ref[which, 0] + other[rows] * table_ref[which, 1]
        turned = (turned * scale[rows]).astype(BF16)
        if which == 0:
            out_ref[h, :, 0:HEAD_DIM] = turned
            continue
        kv = h - keys * group
        for g in range(kv * group, (kv + 1) * group):
            out_ref[g, :, HEAD_DIM : 2 * HEAD_DIM] = turned
            out_ref[g, :, 2 * HEAD_DIM : 3 * HEAD_DIM] = head(v_ref, kv)


def attend_kernel(x_ref, out_ref, value_ref, even_ref, odd_ref):
    length = x_ref.shape[0]
    block = even_ref.shape[0]
    blocks = length // block
    value_ref[:, 0:HEAD_DIM] = x_ref[:, 2 * HEAD_DIM : 3 * HEAD_DIM]
    value_ref[:, HEAD_DIM:] = jnp.ones((length, HEAD_DIM), BF16)
    scale = float(HEAD_DIM ** (-0.5) * np.log2(np.e))

    def score(i, score_ref):
        rows = pl.ds(i * block, block)
        score_ref[...] = dot(x_ref[rows, 0:HEAD_DIM], x_ref[:, HEAD_DIM : 2 * HEAD_DIM], ((1,), (1,)))

    def mix(i, score_ref):
        rows = pl.ds(i * block, block)
        top = jnp.max(score_ref[...], axis=-1, keepdims=True)
        weights = jnp.exp2((score_ref[...] - top) * scale).astype(BF16)
        both = dot(weights, value_ref[...])
        out_ref[rows, :] = (both[:, 0:HEAD_DIM] / both[:, HEAD_DIM:]).astype(BF16)

    score(0, even_ref)

    refs = (even_ref, odd_ref)
    for i in range(blocks):
        if i + 1 < blocks:
            score(i + 1, refs[(i + 1) % 2])
        mix(i, refs[i % 2])


def rms(floats, gain):
    return floats * lax.rsqrt(jnp.mean(floats * floats, axis=-1, keepdims=True) + EPSILON) * gain


def proj_kernel(place_ref, att_ref, w_ref, res_ref, post_ref, pre_ref, ids_ref, *rest):
    *_, out_ref, stream_ref, slot_ref, x_ref = rest
    tokens, width = x_ref.shape
    for h in range(HEADS):
        x_ref[:, h * HEAD_DIM : (h + 1) * HEAD_DIM] = att_ref[h]
    experts = 2 * out_ref.shape[0]
    which = lax.broadcasted_iota(jnp.int32, (experts, tokens), 0)
    first = ids_ref[0:1, :]
    second = ids_ref[1:2, :]
    hit_first = jnp.where(which == first, 1.0, 0.0)
    hit_second = jnp.where(which == second, 1.0, 0.0)
    row = lax.broadcasted_iota(jnp.int32, (tokens, tokens), 0)
    col = lax.broadcasted_iota(jnp.int32, (tokens, tokens), 1)
    before = jnp.where(row < col, 1.0, 0.0).astype(BF16)
    rank = dot((hit_first + hit_second).astype(BF16), before)
    rank_first = jnp.sum(rank * hit_first, axis=0, keepdims=True).astype(jnp.int32)
    rank_second = jnp.sum(rank * hit_second, axis=0, keepdims=True).astype(jnp.int32)
    core = lax.bitwise_and(place_ref[0], 1)

    def slot_of(expert, rank):
        side = lax.bitwise_xor(lax.bitwise_and(expert, 1), core)
        return lax.shift_right_logical(expert, 1) * (2 * CAP) + rank * 2 + side

    slot_first = slot_of(first, rank_first)
    slot_second = slot_of(second, rank_second)
    slot_ref[0:1, :] = slot_first
    slot_ref[1:2, :] = slot_second
    slot = lax.broadcasted_iota(jnp.int32, (experts * CAP, tokens), 0)
    here = (slot == slot_first) | (slot == slot_second)
    picks = jnp.where(here, 1.0, 0.0).astype(BF16)
    mixed = dot(x_ref[...], w_ref[...]).astype(BF16).astype(F32)
    stream = (res_ref[...].astype(F32) + rms(mixed, post_ref[...])).astype(BF16)
    stream_ref[...] = stream
    normed = rms(stream.astype(F32), pre_ref[...]).astype(BF16)
    out_ref[...] = dot(picks, normed).astype(BF16).reshape(out_ref.shape)


def expert_kernel(y_ref, *rest):
    weights, late, (out_ref, wide_ref, x_ref, *held, sems) = list(rest[:3]), rest[3:6], rest[6:]
    copies = [pltpu.make_async_copy(late[i], held[i], sems.at[i]) for i in range(3)]
    for copy in copies:
        copy.start()
    weights += held
    slots, width = y_ref.shape
    sides = [pl.ds(side, slots // 2, stride=2) for side in range(2)]
    blocks = [slice(c * 128, (c + 1) * 128) for c in range(width // 128)]
    for c, cols in enumerate(blocks):
        wide_ref[c] = y_ref[:, cols].astype(F32)
        x_ref[0, :, cols] = wide_ref[c, sides[0], :].astype(BF16)
    for side in range(2):
        gate_ref, up_ref, down_ref = weights[3 * side : 3 * side + 3]
        if side == 1:
            copies[0].wait()
        gated = dot(x_ref[side], gate_ref[...])
        if side == 0:
            for c, cols in enumerate(blocks):
                x_ref[1, :, cols] = wide_ref[c, sides[1], :].astype(BF16)
        if side == 1:
            copies[1].wait()
        lifted = dot(x_ref[side], up_ref[...])
        hidden = (gated / (1.0 + jnp.exp(-gated)) * lifted).astype(BF16)
        if side == 1:
            copies[2].wait()
        made = dot(hidden, down_ref[...])
        for c, cols in enumerate(blocks):
            wide_ref[c, sides[side], :] = made[:, cols]
    for c, cols in enumerate(blocks):
        out_ref[:, cols] = wide_ref[c].astype(BF16)


def combine_kernel(z_ref, stream_ref, slot_ref, weight_ref, share_ref, out_ref):
    slots = z_ref.shape[0]
    tokens, width = stream_ref.shape
    slot = lax.broadcasted_iota(jnp.int32, (slots, tokens), 0)
    picks = [jnp.where(slot == slot_ref[i : i + 1, :], 1.0, 0.0).astype(BF16) for i in range(2)]
    picked = dot(jnp.concatenate(picks, axis=1), z_ref[...], ((0,), (0,)))
    column = lambda row: jnp.broadcast_to(row, (tokens, tokens)).T[:, 0:1]
    weight = weight_ref[...]
    share = share_ref[...]
    weight_first = column(weight * share)
    weight_second = column(weight * (1.0 - share))
    ffn = weight_first * picked[0:tokens] + weight_second * picked[tokens:]
    out_ref[...] = (stream_ref[...].astype(F32) + ffn).astype(BF16)


def local(
    residual_in,
    query_proj,
    key_proj,
    value_proj,
    query_gain,
    key_gain,
    out_weight,
    post_gain,
    pre_gain,
    route_ids,
    group_weight,
    first_share,
    gate_weight,
    up_weight,
    down_weight,
):
    line = ("x", "z")
    sp_count = lax.axis_size(line)
    tokens, width = query_proj.shape[1:]
    length = tokens * sp_count
    chips = sp_count * lax.axis_size("y")
    experts = 2 * chips
    assert sp_count == HEADS and gate_weight.shape[0] == 1 and lax.axis_size("core") == 2
    place = lax.axis_index(("z", "x", "y", "core")).astype(jnp.int32).reshape(1)
    row_table = jnp.asarray(angle_tables(length // GRID_W))
    col_table = jnp.asarray(angle_tables(GRID_W))
    swap_table = jnp.asarray(partner_matrix(), BF16)
    swap = [(0, 1), (1, 0)]
    own = (gate_weight[0], up_weight[0], down_weight[0])
    partner = tuple(lax.ppermute(one, "core", swap) for one in own)

    vmem = pl.BlockSpec(memory_space=pltpu.VMEM)
    smem = pl.BlockSpec(memory_space=pltpu.SMEM)
    limit = lambda mib: pltpu.CompilerParams(vmem_limit_bytes=mib * 2**20)
    kv_width = key_proj.shape[2]
    fixed = lambda *shape: pl.BlockSpec(shape, lambda n: (0,) * len(shape))
    packed = pl.pallas_call(
        pack_kernel,
        grid=(PACK_STEPS,),
        out_shape=jax.ShapeDtypeStruct((HEADS, tokens, 3 * HEAD_DIM), BF16),
        in_specs=[
            smem,
            pl.BlockSpec((tokens, width // PACK_STEPS), lambda n: (0, n)),
            pl.BlockSpec((tokens, kv_width // PACK_STEPS), lambda n: (0, n)),
            pl.BlockSpec((tokens, kv_width // PACK_STEPS), lambda n: (0, n)),
            fixed(1, HEAD_DIM),
            fixed(1, HEAD_DIM),
            fixed(*row_table.shape),
            fixed(*col_table.shape),
            fixed(*swap_table.shape),
        ],
        out_specs=pl.BlockSpec((HEADS // PACK_STEPS, tokens, 3 * HEAD_DIM), lambda n: (n, 0, 0)),
        scratch_shapes=[pltpu.VMEM((2, 2, tokens, HEAD_DIM), F32)],
        compiler_params=limit(63),
        name="pack",
    )(
        place,
        query_proj[0],
        key_proj[0],
        value_proj[0],
        query_gain[None],
        key_gain[None],
        row_table,
        col_table,
        swap_table,
    )
    gathered = lax.all_to_all(packed, line, 0, 0, tiled=True)
    block = 512
    attended = pl.pallas_call(
        attend_kernel,
        out_shape=jax.ShapeDtypeStruct((length, HEAD_DIM), BF16),
        in_specs=[vmem],
        out_specs=vmem,
        scratch_shapes=[
            pltpu.VMEM((length, 2 * HEAD_DIM), BF16),
            pltpu.VMEM((block, length), F32),
            pltpu.VMEM((block, length), F32),
        ],
        compiler_params=limit(24),
        cost_estimate=pl.CostEstimate(
            flops=length * length * HEAD_DIM,
            bytes_accessed=length * HEAD_DIM * 8,
            transcendentals=length * length,
        ),
        name="attend",
    )(gathered.reshape(length, 3 * HEAD_DIM))
    attended = lax.all_to_all(attended.reshape(sp_count, tokens, HEAD_DIM), line, 0, 0, tiled=True)
    hbm = pl.BlockSpec(memory_space=pltpu.HBM)
    sent, stream, slots = pl.pallas_call(
        proj_kernel,
        out_shape=(
            jax.ShapeDtypeStruct((chips, 2 * CAP, width), BF16),
            jax.ShapeDtypeStruct((tokens, width), BF16),
            jax.ShapeDtypeStruct((8, tokens), jnp.int32),
        ),
        in_specs=[smem] + [vmem] * 6 + [hbm] * 3,
        out_specs=(vmem,) * 3,
        scratch_shapes=[
            pltpu.VMEM((tokens, width), BF16),
        ],
        compiler_params=limit(24),
        name="project",
    )(
        place,
        attended,
        out_weight,
        residual_in[0],
        post_gain[None],
        pre_gain[None],
        route_ids[0].T,
        *partner,
    )
    peers = ("z", "x", "y")
    arrived = lax.all_to_all(sent, peers, 0, 0, tiled=True)
    rows = experts * CAP
    answered = pl.pallas_call(
        expert_kernel,
        out_shape=jax.ShapeDtypeStruct((rows, width), BF16),
        in_specs=[vmem] * 4 + [hbm] * 3,
        out_specs=vmem,
        scratch_shapes=[
            pltpu.VMEM((width // 128, rows, 128), F32),
            pltpu.VMEM((2, rows // 2, width), BF16),
            *[pltpu.VMEM(one.shape, BF16) for one in partner],
            pltpu.SemaphoreType.DMA((3,)),
        ],
        compiler_params=limit(24),
        name="expert",
    )(arrived.reshape(rows, width), *own, *partner)
    returned = lax.all_to_all(answered.reshape(chips, 2 * CAP, width), peers, 0, 0, tiled=True)
    combined = pl.pallas_call(
        combine_kernel,
        out_shape=jax.ShapeDtypeStruct((tokens, width), BF16),
        in_specs=[vmem] * 5,
        out_specs=vmem,
        compiler_params=limit(16),
        name="combine",
    )(returned.reshape(rows, width), stream, slots, group_weight, first_share)
    return combined[None]


def solution(mesh):
    assert mesh.devices.shape == (16, 8)
    grid = mesh.devices.reshape(4, 4, 4, 2)
    mesh = Mesh(grid, ("z", "x", "y", "core"))
    placed = (
        P(("y", "core"), ("z", "x"), None),
        P(("y", "core"), ("z", "x"), None),
        P(("y", "core"), ("z", "x"), None),
        P(("y", "core"), ("z", "x"), None),
        P(),
        P(),
        P(),
        P(),
        P(),
        P(("y", "core"), ("z", "x"), None),
        P(("y", "core"), ("z", "x")),
        P(("y", "core"), ("z", "x")),
        P(("z", "x", "y", "core"), None, None),
        P(("z", "x", "y", "core"), None, None),
        P(("z", "x", "y", "core"), None, None),
    )
    return jax.shard_map(
        local, mesh=mesh, in_specs=placed, out_specs=P(("y", "core"), ("z", "x"), None), check_vma=False
    )
```

```python
import functools

import jax
import jax.numpy as jnp
import numpy as np
from jax import lax
from jax.experimental import pallas as pl
from jax.experimental.pallas import tpu as pltpu
from jax.sharding import Mesh
from jax.sharding import PartitionSpec as P

HEADS = 16
KV_HEADS = 4
HEAD_DIM = 128
GRID_W = 64
CAP = 4
EPSILON = 1e-06
LATE_CORE = 0
PACK_STEPS = 2
STAGGER_NS = 8200
F32 = jnp.float32
BF16 = jnp.bfloat16


def dot(a, b, dims=((1,), (0,))):
    return lax.dot_general(a, b, (dims, ((), ())), preferred_element_type=F32)


def angle_tables(count):
    quarter = HEAD_DIM // 4
    inverse = np.float32(10000.0) ** (-np.arange(quarter, dtype=np.float32) / np.float32(quarter))
    angles = np.arange(count, dtype=np.float32)[:, None] * inverse.astype(np.float32)
    angles = np.tile(angles.astype(np.float64), (1, 4))
    return np.stack([np.cos(angles), np.sin(angles)]).astype(np.float32)


def partner_matrix():
    lane = np.arange(HEAD_DIM)
    low = (lane & 32) == 0
    matrix = np.zeros((HEAD_DIM, HEAD_DIM), np.float32)
    matrix[np.where(low, lane + 32, lane - 32), lane] = np.where(low, -1.0, 1.0)
    return matrix


def pack_kernel(
    place_ref, q_ref, k_ref, v_ref, qg_ref, kg_ref, row_ref, col_ref, swap_ref, out_ref, table_ref
):
    tokens = k_ref.shape[0]
    late = lax.bitwise_and(place_ref[0], 1) == LATE_CORE

    @pl.when((pl.program_id(0) == 0) & late)
    def _():
        pl.delay(STAGGER_NS)

    @pl.when(pl.program_id(0) == 0)
    def _():
        lane = lax.broadcasted_iota(jnp.int32, (GRID_W, HEAD_DIM), 1)
        line = lax.broadcasted_iota(jnp.int32, (1, HEAD_DIM), 1)
        low = lax.bitwise_and(line, 32) == 0
        start = lax.shift_right_logical(place_ref[0], 3) * (tokens // GRID_W)
        for which, gain_ref in enumerate((qg_ref, kg_ref)):
            gain = gain_ref[...]
            wide = jnp.broadcast_to(gain, (8, HEAD_DIM))
            other = jnp.where(low, pltpu.roll(wide, 96, 1)[0:1], pltpu.roll(wide, 32, 1)[0:1])
            for kind, scale in enumerate((gain, other)):
                for i in range(tokens // GRID_W):
                    at_row = row_ref[kind, pl.ds(start + i, 1), :]
                    table = jnp.where(lane < HEAD_DIM // 2, at_row, col_ref[kind])
                    table_ref[which, kind, i * GRID_W : (i + 1) * GRID_W, :] = table * scale

    ones = jnp.ones((HEAD_DIM, HEAD_DIM), BF16)
    keys = k_ref.shape[1] // HEAD_DIM
    group = HEADS // KV_HEADS
    head = lambda ref, h: ref[:, h * HEAD_DIM : (h + 1) * HEAD_DIM]
    raw = [head(q_ref, h) for h in range(keys * group)] + [head(k_ref, kv) for kv in range(keys)]
    raw = jnp.concatenate(raw, axis=0)
    floats = raw.astype(F32)
    square = floats * floats
    high = square.astype(BF16)
    low_part = (square - high.astype(F32)).astype(BF16)
    total = dot(high, ones) + dot(low_part, ones)
    scale = lax.rsqrt(total * (1.0 / HEAD_DIM) + EPSILON)
    other = dot(raw, swap_ref[...])
    for h in range(keys * (group + 1)):
        rows = slice(h * tokens, (h + 1) * tokens)
        which = 1 if h >= keys * group else 0
        turned = floats[rows] * table_ref[which, 0] + other[rows] * table_ref[which, 1]
        turned = (turned * scale[rows]).astype(BF16)
        if which == 0:
            out_ref[h, :, 0:HEAD_DIM] = turned
            continue
        kv = h - keys * group
        for g in range(kv * group, (kv + 1) * group):
            out_ref[g, :, HEAD_DIM : 2 * HEAD_DIM] = turned
            out_ref[g, :, 2 * HEAD_DIM : 3 * HEAD_DIM] = head(v_ref, kv)


def attend_kernel(x_ref, out_ref, value_ref, even_ref, odd_ref):
    length = x_ref.shape[0]
    block = even_ref.shape[0]
    blocks = length // block
    value_ref[:, 0:HEAD_DIM] = x_ref[:, 2 * HEAD_DIM : 3 * HEAD_DIM]
    value_ref[:, HEAD_DIM:] = jnp.ones((length, HEAD_DIM), BF16)
    scale = float(HEAD_DIM ** (-0.5) * np.log2(np.e))

    def score(i, score_ref):
        rows = pl.ds(i * block, block)
        score_ref[...] = dot(x_ref[rows, 0:HEAD_DIM], x_ref[:, HEAD_DIM : 2 * HEAD_DIM], ((1,), (1,)))

    def mix(i, score_ref):
        rows = pl.ds(i * block, block)
        top = jnp.max(score_ref[...], axis=-1, keepdims=True)
        weights = jnp.exp2((score_ref[...] - top) * scale).astype(BF16)
        both = dot(weights, value_ref[...])
        out_ref[rows, :] = (both[:, 0:HEAD_DIM] / both[:, HEAD_DIM:]).astype(BF16)

    score(0, even_ref)

    refs = (even_ref, odd_ref)
    for i in range(blocks):
        if i + 1 < blocks:
            score(i + 1, refs[(i + 1) % 2])
        mix(i, refs[i % 2])


def rms(floats, gain):
    return floats * lax.rsqrt(jnp.mean(floats * floats, axis=-1, keepdims=True) + EPSILON) * gain


def proj_kernel(place_ref, att_ref, w_ref, res_ref, post_ref, pre_ref, ids_ref, weight_ref, share_ref, *rest):
    *_, out_ref, stream_ref, slot_ref, scale_ref, x_ref = rest
    tokens, width = x_ref.shape
    weight = weight_ref[...]
    share = share_ref[...]
    top = lax.broadcasted_iota(jnp.int32, (tokens, tokens), 0) == 0
    scale_ref[...] = jnp.where(top, weight * share, weight * (1.0 - share)).T
    for h in range(HEADS):
        x_ref[:, h * HEAD_DIM : (h + 1) * HEAD_DIM] = att_ref[h]
    experts = 2 * out_ref.shape[0]
    which = lax.broadcasted_iota(jnp.int32, (experts, tokens), 0)
    first = ids_ref[0:1, :]
    second = ids_ref[1:2, :]
    hit_first = jnp.where(which == first, 1.0, 0.0)
    hit_second = jnp.where(which == second, 1.0, 0.0)
    row = lax.broadcasted_iota(jnp.int32, (tokens, tokens), 0)
    col = lax.broadcasted_iota(jnp.int32, (tokens, tokens), 1)
    before = jnp.where(row < col, 1.0, 0.0).astype(BF16)
    rank = dot((hit_first + hit_second).astype(BF16), before)
    rank_first = jnp.sum(rank * hit_first, axis=0, keepdims=True).astype(jnp.int32)
    rank_second = jnp.sum(rank * hit_second, axis=0, keepdims=True).astype(jnp.int32)
    core = lax.bitwise_and(place_ref[0], 1)

    def slot_of(expert, rank):
        side = lax.bitwise_xor(lax.bitwise_and(expert, 1), core)
        return lax.shift_right_logical(expert, 1) * (2 * CAP) + rank * 2 + side

    slot_first = slot_of(first, rank_first)
    slot_second = slot_of(second, rank_second)
    slot_ref[0:1, :] = slot_first
    slot_ref[1:2, :] = slot_second
    slot = lax.broadcasted_iota(jnp.int32, (experts * CAP, tokens), 0)
    here = (slot == slot_first) | (slot == slot_second)
    picks = jnp.where(here, 1.0, 0.0).astype(BF16)
    mixed = dot(x_ref[...], w_ref[...]).astype(BF16).astype(F32)
    stream = (res_ref[...].astype(F32) + rms(mixed, post_ref[...])).astype(BF16)
    stream_ref[...] = stream
    normed = rms(stream.astype(F32), pre_ref[...]).astype(BF16)
    out_ref[...] = dot(picks, normed).astype(BF16).reshape(out_ref.shape)


def expert_kernel(y_ref, *rest):
    weights, late, (out_ref, wide_ref, x_ref, *held, sems) = list(rest[:3]), rest[3:6], rest[6:]
    copies = [pltpu.make_async_copy(late[i], held[i], sems.at[i]) for i in range(3)]
    for copy in copies:
        copy.start()
    weights += held
    slots, width = y_ref.shape
    sides = [pl.ds(side, slots // 2, stride=2) for side in range(2)]
    blocks = [slice(c * 128, (c + 1) * 128) for c in range(width // 128)]
    for c, cols in enumerate(blocks):
        wide_ref[c] = y_ref[:, cols].astype(F32)
        x_ref[0, :, cols] = wide_ref[c, sides[0], :].astype(BF16)
    for side in range(2):
        gate_ref, up_ref, down_ref = weights[3 * side : 3 * side + 3]
        if side == 1:
            copies[0].wait()
        gated = dot(x_ref[side], gate_ref[...])
        if side == 0:
            for c, cols in enumerate(blocks):
                x_ref[1, :, cols] = wide_ref[c, sides[1], :].astype(BF16)
        if side == 1:
            copies[1].wait()
        lifted = dot(x_ref[side], up_ref[...])
        hidden = (gated / (1.0 + jnp.exp(-gated)) * lifted).astype(BF16)
        if side == 1:
            copies[2].wait()
        made = dot(hidden, down_ref[...])
        for c, cols in enumerate(blocks):
            wide_ref[c, sides[side], :] = made[:, cols]
    for c, cols in enumerate(blocks):
        out_ref[:, cols] = wide_ref[c].astype(BF16)


def combine_kernel(z_ref, stream_ref, slot_ref, scale_ref, out_ref):
    slots = z_ref.shape[0]
    tokens, width = stream_ref.shape
    slot = lax.broadcasted_iota(jnp.int32, (slots, tokens), 0)
    picks = [jnp.where(slot == slot_ref[i : i + 1, :], 1.0, 0.0).astype(BF16) for i in range(2)]
    picked = dot(jnp.concatenate(picks, axis=1), z_ref[...], ((0,), (0,)))
    ffn = scale_ref[:, 0:1] * picked[0:tokens] + scale_ref[:, 1:2] * picked[tokens:]
    out_ref[...] = (stream_ref[...].astype(F32) + ffn).astype(BF16)


def local(
    residual_in,
    query_proj,
    key_proj,
    value_proj,
    query_gain,
    key_gain,
    out_weight,
    post_gain,
    pre_gain,
    route_ids,
    group_weight,
    first_share,
    gate_weight,
    up_weight,
    down_weight,
):
    line = ("x", "z")
    sp_count = lax.axis_size(line)
    tokens, width = query_proj.shape[1:]
    length = tokens * sp_count
    chips = sp_count * lax.axis_size("y")
    experts = 2 * chips
    assert sp_count == HEADS and gate_weight.shape[0] == 1 and lax.axis_size("core") == 2
    place = lax.axis_index(("z", "x", "y", "core")).astype(jnp.int32).reshape(1)
    row_table = jnp.asarray(angle_tables(length // GRID_W))
    col_table = jnp.asarray(angle_tables(GRID_W))
    swap_table = jnp.asarray(partner_matrix(), BF16)
    swap = [(0, 1), (1, 0)]
    own = (gate_weight[0], up_weight[0], down_weight[0])
    partner = tuple(lax.ppermute(one, "core", swap) for one in own)

    vmem = pl.BlockSpec(memory_space=pltpu.VMEM)
    smem = pl.BlockSpec(memory_space=pltpu.SMEM)
    limit = lambda mib: pltpu.CompilerParams(vmem_limit_bytes=mib * 2**20)
    kv_width = key_proj.shape[2]
    fixed = lambda *shape: pl.BlockSpec(shape, lambda n: (0,) * len(shape))
    packed = pl.pallas_call(
        pack_kernel,
        grid=(PACK_STEPS,),
        out_shape=jax.ShapeDtypeStruct((HEADS, tokens, 3 * HEAD_DIM), BF16),
        in_specs=[
            smem,
            pl.BlockSpec((tokens, width // PACK_STEPS), lambda n: (0, n)),
            pl.BlockSpec((tokens, kv_width // PACK_STEPS), lambda n: (0, n)),
            pl.BlockSpec((tokens, kv_width // PACK_STEPS), lambda n: (0, n)),
            fixed(1, HEAD_DIM),
            fixed(1, HEAD_DIM),
            fixed(*row_table.shape),
            fixed(*col_table.shape),
            fixed(*swap_table.shape),
        ],
        out_specs=pl.BlockSpec((HEADS // PACK_STEPS, tokens, 3 * HEAD_DIM), lambda n: (n, 0, 0)),
        scratch_shapes=[pltpu.VMEM((2, 2, tokens, HEAD_DIM), F32)],
        compiler_params=limit(63),
        name="pack",
    )(
        place,
        query_proj[0],
        key_proj[0],
        value_proj[0],
        query_gain[None],
        key_gain[None],
        row_table,
        col_table,
        swap_table,
    )
    gathered = lax.all_to_all(packed, line, 0, 0, tiled=True)
    block = 512
    attended = pl.pallas_call(
        attend_kernel,
        out_shape=jax.ShapeDtypeStruct((length, HEAD_DIM), BF16),
        in_specs=[vmem],
        out_specs=vmem,
        scratch_shapes=[
            pltpu.VMEM((length, 2 * HEAD_DIM), BF16),
            pltpu.VMEM((block, length), F32),
            pltpu.VMEM((block, length), F32),
        ],
        compiler_params=limit(24),
        cost_estimate=pl.CostEstimate(
            flops=length * length * HEAD_DIM,
            bytes_accessed=length * HEAD_DIM * 8,
            transcendentals=length * length,
        ),
        name="attend",
    )(gathered.reshape(length, 3 * HEAD_DIM))
    attended = lax.all_to_all(attended.reshape(sp_count, tokens, HEAD_DIM), line, 0, 0, tiled=True)
    hbm = pl.BlockSpec(memory_space=pltpu.HBM)
    sent, stream, slots, scales = pl.pallas_call(
        proj_kernel,
        out_shape=(
            jax.ShapeDtypeStruct((chips, 2 * CAP, width), BF16),
            jax.ShapeDtypeStruct((tokens, width), BF16),
            jax.ShapeDtypeStruct((8, tokens), jnp.int32),
            jax.ShapeDtypeStruct((tokens, tokens), F32),
        ),
        in_specs=[smem] + [vmem] * 8 + [hbm] * 3,
        out_specs=(vmem,) * 4,
        scratch_shapes=[
            pltpu.VMEM((tokens, width), BF16),
        ],
        compiler_params=limit(24),
        name="project",
    )(
        place,
        attended,
        out_weight,
        residual_in[0],
        post_gain[None],
        pre_gain[None],
        route_ids[0].T,
        group_weight,
        first_share,
        *partner,
    )
    peers = ("z", "x", "y")
    arrived = lax.all_to_all(sent, peers, 0, 0, tiled=True)
    rows = experts * CAP
    answered = pl.pallas_call(
        expert_kernel,
        out_shape=jax.ShapeDtypeStruct((rows, width), BF16),
        in_specs=[vmem] * 4 + [hbm] * 3,
        out_specs=vmem,
        scratch_shapes=[
            pltpu.VMEM((width // 128, rows, 128), F32),
            pltpu.VMEM((2, rows // 2, width), BF16),
            *[pltpu.VMEM(one.shape, BF16) for one in partner],
            pltpu.SemaphoreType.DMA((3,)),
        ],
        compiler_params=limit(24),
        name="expert",
    )(arrived.reshape(rows, width), *own, *partner)
    returned = lax.all_to_all(answered.reshape(chips, 2 * CAP, width), peers, 0, 0, tiled=True)
    combined = pl.pallas_call(
        combine_kernel,
        out_shape=jax.ShapeDtypeStruct((tokens, width), BF16),
        in_specs=[vmem] * 4,
        out_specs=vmem,
        compiler_params=limit(16),
        name="combine",
    )(returned.reshape(rows, width), stream, slots, scales)
    return combined[None]


def solution(mesh):
    assert mesh.devices.shape == (16, 8)
    grid = mesh.devices.reshape(4, 4, 4, 2)
    mesh = Mesh(grid, ("z", "x", "y", "core"))
    placed = (
        P(("y", "core"), ("z", "x"), None),
        P(("y", "core"), ("z", "x"), None),
        P(("y", "core"), ("z", "x"), None),
        P(("y", "core"), ("z", "x"), None),
        P(),
        P(),
        P(),
        P(),
        P(),
        P(("y", "core"), ("z", "x"), None),
        P(("y", "core"), ("z", "x")),
        P(("y", "core"), ("z", "x")),
        P(("z", "x", "y", "core"), None, None),
        P(("z", "x", "y", "core"), None, None),
        P(("z", "x", "y", "core"), None, None),
    )
    return jax.shard_map(
        local, mesh=mesh, in_specs=placed, out_specs=P(("y", "core"), ("z", "x"), None), check_vma=False
    )
```

```python
import functools

import jax
import jax.numpy as jnp
import numpy as np
from jax import lax
from jax.experimental import pallas as pl
from jax.experimental.pallas import tpu as pltpu
from jax.sharding import Mesh
from jax.sharding import PartitionSpec as P

HEADS = 16
KV_HEADS = 4
HEAD_DIM = 128
GRID_W = 64
CAP = 4
EPSILON = 1e-06
LATE_CORE = 0
PACK_STEPS = 1
STAGGER_NS = 8200
F32 = jnp.float32
BF16 = jnp.bfloat16


def dot(a, b, dims=((1,), (0,))):
    return lax.dot_general(a, b, (dims, ((), ())), preferred_element_type=F32)


def angle_tables(count):
    quarter = HEAD_DIM // 4
    inverse = np.float32(10000.0) ** (-np.arange(quarter, dtype=np.float32) / np.float32(quarter))
    angles = np.arange(count, dtype=np.float32)[:, None] * inverse.astype(np.float32)
    angles = np.tile(angles.astype(np.float64), (1, 4))
    return np.stack([np.cos(angles), np.sin(angles)]).astype(np.float32)


def partner_matrix():
    lane = np.arange(HEAD_DIM)
    low = (lane & 32) == 0
    matrix = np.zeros((HEAD_DIM, HEAD_DIM), np.float32)
    matrix[np.where(low, lane + 32, lane - 32), lane] = np.where(low, -1.0, 1.0)
    return matrix


def pack_kernel(
    place_ref, q_ref, k_ref, v_ref, qg_ref, kg_ref, row_ref, col_ref, swap_ref, out_ref, table_ref
):
    tokens = k_ref.shape[0]
    late = lax.bitwise_and(place_ref[0], 1) == LATE_CORE

    @pl.when((pl.program_id(0) == 0) & late)
    def _():
        pl.delay(STAGGER_NS)

    @pl.when(pl.program_id(0) == 0)
    def _():
        lane = lax.broadcasted_iota(jnp.int32, (GRID_W, HEAD_DIM), 1)
        line = lax.broadcasted_iota(jnp.int32, (1, HEAD_DIM), 1)
        low = lax.bitwise_and(line, 32) == 0
        start = lax.shift_right_logical(place_ref[0], 3) * (tokens // GRID_W)
        for which, gain_ref in enumerate((qg_ref, kg_ref)):
            gain = gain_ref[...]
            wide = jnp.broadcast_to(gain, (8, HEAD_DIM))
            other = jnp.where(low, pltpu.roll(wide, 96, 1)[0:1], pltpu.roll(wide, 32, 1)[0:1])
            for kind, scale in enumerate((gain, other)):
                for i in range(tokens // GRID_W):
                    at_row = row_ref[kind, pl.ds(start + i, 1), :]
                    table = jnp.where(lane < HEAD_DIM // 2, at_row, col_ref[kind])
                    table_ref[which, kind, i * GRID_W : (i + 1) * GRID_W, :] = table * scale

    ones = jnp.ones((HEAD_DIM, HEAD_DIM), BF16)
    keys = k_ref.shape[1] // HEAD_DIM
    group = HEADS // KV_HEADS
    head = lambda ref, h: ref[:, h * HEAD_DIM : (h + 1) * HEAD_DIM]
    raw = [head(q_ref, h) for h in range(keys * group)] + [head(k_ref, kv) for kv in range(keys)]
    raw = jnp.concatenate(raw, axis=0)
    floats = raw.astype(F32)
    square = floats * floats
    high = square.astype(BF16)
    low_part = (square - high.astype(F32)).astype(BF16)
    total = dot(high, ones) + dot(low_part, ones)
    scale = lax.rsqrt(total * (1.0 / HEAD_DIM) + EPSILON)
    other = dot(raw, swap_ref[...])
    for h in range(keys * (group + 1)):
        rows = slice(h * tokens, (h + 1) * tokens)
        which = 1 if h >= keys * group else 0
        turned = floats[rows] * table_ref[which, 0] + other[rows] * table_ref[which, 1]
        turned = (turned * scale[rows]).astype(BF16)
        if which == 0:
            out_ref[h, :, 0:HEAD_DIM] = turned
            continue
        kv = h - keys * group
        for g in range(kv * group, (kv + 1) * group):
            out_ref[g, :, HEAD_DIM : 2 * HEAD_DIM] = turned
            out_ref[g, :, 2 * HEAD_DIM : 3 * HEAD_DIM] = head(v_ref, kv)


def attend_kernel(x_ref, out_ref, value_ref, even_ref, odd_ref):
    length = x_ref.shape[0]
    block = even_ref.shape[0]
    blocks = length // block
    value_ref[:, 0:HEAD_DIM] = x_ref[:, 2 * HEAD_DIM : 3 * HEAD_DIM]
    value_ref[:, HEAD_DIM:] = jnp.ones((length, HEAD_DIM), BF16)
    scale = float(HEAD_DIM ** (-0.5) * np.log2(np.e))

    def score(i, score_ref):
        rows = pl.ds(i * block, block)
        score_ref[...] = dot(x_ref[rows, 0:HEAD_DIM], x_ref[:, HEAD_DIM : 2 * HEAD_DIM], ((1,), (1,)))

    def mix(i, score_ref):
        rows = pl.ds(i * block, block)
        top = jnp.max(score_ref[...], axis=-1, keepdims=True)
        weights = jnp.exp2((score_ref[...] - top) * scale).astype(BF16)
        both = dot(weights, value_ref[...])
        out_ref[rows, :] = (both[:, 0:HEAD_DIM] / both[:, HEAD_DIM:]).astype(BF16)

    score(0, even_ref)

    refs = (even_ref, odd_ref)
    for i in range(blocks):
        if i + 1 < blocks:
            score(i + 1, refs[(i + 1) % 2])
        mix(i, refs[i % 2])


def rms(floats, gain):
    return floats * lax.rsqrt(jnp.mean(floats * floats, axis=-1, keepdims=True) + EPSILON) * gain


def proj_kernel(place_ref, att_ref, w_ref, res_ref, post_ref, pre_ref, ids_ref, *rest):
    *_, out_ref, stream_ref, slot_ref, x_ref = rest
    tokens, width = x_ref.shape
    for h in range(HEADS):
        x_ref[:, h * HEAD_DIM : (h + 1) * HEAD_DIM] = att_ref[h]
    experts = 2 * out_ref.shape[0]
    which = lax.broadcasted_iota(jnp.int32, (experts, tokens), 0)
    first = ids_ref[0:1, :]
    second = ids_ref[1:2, :]
    hit_first = jnp.where(which == first, 1.0, 0.0)
    hit_second = jnp.where(which == second, 1.0, 0.0)
    row = lax.broadcasted_iota(jnp.int32, (tokens, tokens), 0)
    col = lax.broadcasted_iota(jnp.int32, (tokens, tokens), 1)
    before = jnp.where(row < col, 1.0, 0.0).astype(BF16)
    rank = dot((hit_first + hit_second).astype(BF16), before)
    rank_first = jnp.sum(rank * hit_first, axis=0, keepdims=True).astype(jnp.int32)
    rank_second = jnp.sum(rank * hit_second, axis=0, keepdims=True).astype(jnp.int32)
    core = lax.bitwise_and(place_ref[0], 1)

    def slot_of(expert, rank):
        side = lax.bitwise_xor(lax.bitwise_and(expert, 1), core)
        return lax.shift_right_logical(expert, 1) * (2 * CAP) + rank * 2 + side

    slot_first = slot_of(first, rank_first)
    slot_second = slot_of(second, rank_second)
    slot_ref[0:1, :] = slot_first
    slot_ref[1:2, :] = slot_second
    slot = lax.broadcasted_iota(jnp.int32, (experts * CAP, tokens), 0)
    here = (slot == slot_first) | (slot == slot_second)
    picks = jnp.where(here, 1.0, 0.0).astype(BF16)
    mixed = dot(x_ref[...], w_ref[...]).astype(BF16).astype(F32)
    stream = (res_ref[...].astype(F32) + rms(mixed, post_ref[...])).astype(BF16)
    stream_ref[...] = stream
    normed = rms(stream.astype(F32), pre_ref[...]).astype(BF16)
    out_ref[...] = dot(picks, normed).astype(BF16).reshape(out_ref.shape)


def expert_kernel(y_ref, *rest):
    weights, late, (out_ref, wide_ref, x_ref, *held, sems) = list(rest[:3]), rest[3:6], rest[6:]
    copies = [pltpu.make_async_copy(late[i], held[i], sems.at[i]) for i in range(3)]
    for copy in copies:
        copy.start()
    weights += held
    slots, width = y_ref.shape
    sides = [pl.ds(side, slots // 2, stride=2) for side in range(2)]
    blocks = [slice(c * 128, (c + 1) * 128) for c in range(width // 128)]
    for c, cols in enumerate(blocks):
        wide_ref[c] = y_ref[:, cols].astype(F32)
        x_ref[0, :, cols] = wide_ref[c, sides[0], :].astype(BF16)
    for side in range(2):
        gate_ref, up_ref, down_ref = weights[3 * side : 3 * side + 3]
        if side == 1:
            copies[0].wait()
        gated = dot(x_ref[side], gate_ref[...])
        if side == 0:
            for c, cols in enumerate(blocks):
                x_ref[1, :, cols] = wide_ref[c, sides[1], :].astype(BF16)
        if side == 1:
            copies[1].wait()
        lifted = dot(x_ref[side], up_ref[...])
        hidden = (gated / (1.0 + jnp.exp(-gated)) * lifted).astype(BF16)
        if side == 1:
            copies[2].wait()
        made = dot(hidden, down_ref[...])
        for c, cols in enumerate(blocks):
            wide_ref[c, sides[side], :] = made[:, cols]
    for c, cols in enumerate(blocks):
        out_ref[:, cols] = wide_ref[c].astype(BF16)


def combine_kernel(z_ref, stream_ref, slot_ref, weight_ref, share_ref, out_ref):
    slots = z_ref.shape[0]
    tokens, width = stream_ref.shape
    slot = lax.broadcasted_iota(jnp.int32, (slots, tokens), 0)
    picks = [jnp.where(slot == slot_ref[i : i + 1, :], 1.0, 0.0).astype(BF16) for i in range(2)]
    picked = dot(jnp.concatenate(picks, axis=1), z_ref[...], ((0,), (0,)))
    column = lambda row: jnp.broadcast_to(row, (tokens, tokens)).T[:, 0:1]
    weight = weight_ref[...]
    share = share_ref[...]
    weight_first = column(weight * share)
    weight_second = column(weight * (1.0 - share))
    ffn = weight_first * picked[0:tokens] + weight_second * picked[tokens:]
    out_ref[...] = (stream_ref[...].astype(F32) + ffn).astype(BF16)


def local(
    residual_in,
    query_proj,
    key_proj,
    value_proj,
    query_gain,
    key_gain,
    out_weight,
    post_gain,
    pre_gain,
    route_ids,
    group_weight,
    first_share,
    gate_weight,
    up_weight,
    down_weight,
):
    line = ("x", "z")
    sp_count = lax.axis_size(line)
    tokens, width = query_proj.shape[1:]
    length = tokens * sp_count
    chips = sp_count * lax.axis_size("y")
    experts = 2 * chips
    assert sp_count == HEADS and gate_weight.shape[0] == 1 and lax.axis_size("core") == 2
    place = lax.axis_index(("z", "x", "y", "core")).astype(jnp.int32).reshape(1)
    row_table = jnp.asarray(angle_tables(length // GRID_W))
    col_table = jnp.asarray(angle_tables(GRID_W))
    swap_table = jnp.asarray(partner_matrix(), BF16)
    swap = [(0, 1), (1, 0)]
    own = (gate_weight[0], up_weight[0], down_weight[0])
    partner = tuple(lax.ppermute(one, "core", swap) for one in own)

    vmem = pl.BlockSpec(memory_space=pltpu.VMEM)
    smem = pl.BlockSpec(memory_space=pltpu.SMEM)
    limit = lambda mib: pltpu.CompilerParams(vmem_limit_bytes=mib * 2**20)
    kv_width = key_proj.shape[2]
    fixed = lambda *shape: pl.BlockSpec(shape, lambda n: (0,) * len(shape))
    packed = pl.pallas_call(
        pack_kernel,
        grid=(PACK_STEPS,),
        out_shape=jax.ShapeDtypeStruct((HEADS, tokens, 3 * HEAD_DIM), BF16),
        in_specs=[
            smem,
            pl.BlockSpec((tokens, width // PACK_STEPS), lambda n: (0, n)),
            pl.BlockSpec((tokens, kv_width // PACK_STEPS), lambda n: (0, n)),
            pl.BlockSpec((tokens, kv_width // PACK_STEPS), lambda n: (0, n)),
            fixed(1, HEAD_DIM),
            fixed(1, HEAD_DIM),
            fixed(*row_table.shape),
            fixed(*col_table.shape),
            fixed(*swap_table.shape),
        ],
        out_specs=pl.BlockSpec((HEADS // PACK_STEPS, tokens, 3 * HEAD_DIM), lambda n: (n, 0, 0)),
        scratch_shapes=[pltpu.VMEM((2, 2, tokens, HEAD_DIM), F32)],
        compiler_params=limit(63),
        name="pack",
    )(
        place,
        query_proj[0],
        key_proj[0],
        value_proj[0],
        query_gain[None],
        key_gain[None],
        row_table,
        col_table,
        swap_table,
    )
    gathered = lax.all_to_all(packed, line, 0, 0, tiled=True)
    block = 512
    attended = pl.pallas_call(
        attend_kernel,
        out_shape=jax.ShapeDtypeStruct((length, HEAD_DIM), BF16),
        in_specs=[vmem],
        out_specs=vmem,
        scratch_shapes=[
            pltpu.VMEM((length, 2 * HEAD_DIM), BF16),
            pltpu.VMEM((block, length), F32),
            pltpu.VMEM((block, length), F32),
        ],
        compiler_params=limit(24),
        cost_estimate=pl.CostEstimate(
            flops=length * length * HEAD_DIM,
            bytes_accessed=length * HEAD_DIM * 8,
            transcendentals=length * length,
        ),
        name="attend",
    )(gathered.reshape(length, 3 * HEAD_DIM))
    attended = lax.all_to_all(attended.reshape(sp_count, tokens, HEAD_DIM), line, 0, 0, tiled=True)
    hbm = pl.BlockSpec(memory_space=pltpu.HBM)
    sent, stream, slots = pl.pallas_call(
        proj_kernel,
        out_shape=(
            jax.ShapeDtypeStruct((chips, 2 * CAP, width), BF16),
            jax.ShapeDtypeStruct((tokens, width), BF16),
            jax.ShapeDtypeStruct((8, tokens), jnp.int32),
        ),
        in_specs=[smem] + [vmem] * 6 + [hbm] * 3,
        out_specs=(vmem,) * 3,
        scratch_shapes=[
            pltpu.VMEM((tokens, width), BF16),
        ],
        compiler_params=limit(24),
        name="project",
    )(
        place,
        attended,
        out_weight,
        residual_in[0],
        post_gain[None],
        pre_gain[None],
        route_ids[0].T,
        *partner,
    )
    peers = ("z", "x", "y")
    arrived = lax.all_to_all(sent, peers, 0, 0, tiled=True)
    rows = experts * CAP
    answered = pl.pallas_call(
        expert_kernel,
        out_shape=jax.ShapeDtypeStruct((rows, width), BF16),
        in_specs=[vmem] * 4 + [hbm] * 3,
        out_specs=vmem,
        scratch_shapes=[
            pltpu.VMEM((width // 128, rows, 128), F32),
            pltpu.VMEM((2, rows // 2, width), BF16),
            *[pltpu.VMEM(one.shape, BF16) for one in partner],
            pltpu.SemaphoreType.DMA((3,)),
        ],
        compiler_params=limit(24),
        name="expert",
    )(arrived.reshape(rows, width), *own, *partner)
    returned = lax.all_to_all(answered.reshape(chips, 2 * CAP, width), peers, 0, 0, tiled=True)
    combined = pl.pallas_call(
        combine_kernel,
        out_shape=jax.ShapeDtypeStruct((tokens, width), BF16),
        in_specs=[vmem] * 5,
        out_specs=vmem,
        compiler_params=limit(16),
        name="combine",
    )(returned.reshape(rows, width), stream, slots, group_weight, first_share)
    return combined[None]


def solution(mesh):
    assert mesh.devices.shape == (16, 8)
    grid = mesh.devices.reshape(4, 4, 4, 2)
    mesh = Mesh(grid, ("z", "x", "y", "core"))
    placed = (
        P(("y", "core"), ("z", "x"), None),
        P(("y", "core"), ("z", "x"), None),
        P(("y", "core"), ("z", "x"), None),
        P(("y", "core"), ("z", "x"), None),
        P(),
        P(),
        P(),
        P(),
        P(),
        P(("y", "core"), ("z", "x"), None),
        P(("y", "core"), ("z", "x")),
        P(("y", "core"), ("z", "x")),
        P(("z", "x", "y", "core"), None, None),
        P(("z", "x", "y", "core"), None, None),
        P(("z", "x", "y", "core"), None, None),
    )
    return jax.shard_map(
        local, mesh=mesh, in_specs=placed, out_specs=P(("y", "core"), ("z", "x"), None), check_vma=False
    )
```
